512 devices in a mesh: fs: 128 (over z, x, core), tp: 4 (over y).
Axes of the slice: x: 4, y: 4, z: 16, core: 2. Of those that a mesh axis runs over, the one named last changes fastest.
Arguments:
- inputs: bfloat16 [16384, 2048], P('fs', 'tp'), may hold values from -24 to 24
- query_grad: bfloat16 [16384, 1024], P('fs', 'tp'), may hold values from -6 to 6
- forget_grad: bfloat16 [16384, 1024], P('fs', 'tp'), may hold values from -6 to 6
- forget_pre: bfloat16 [16384, 1024], P('fs', 'tp'), may hold values from -8 to 8
- lower_bound: float32 [1024], P('tp'), may hold values from 0.1 to 0.9
- query_weight: float32 [2048, 1024], P('fs', 'tp'), may hold values from -0.125 to 0.125
- forget_weight: float32 [2048, 1024], P('fs', 'tp'), may hold values from -0.125 to 0.125
- query_moment: float32 [2048, 1024], P('fs', 'tp'), may hold values from -6 to 6
- forget_moment: float32 [2048, 1024], P('fs', 'tp'), may hold values from -6 to 6
- query_rows: float32 [2048, 2048], P('fs'), may hold values from -0.6 to 0.6
- forget_rows: float32 [2048, 2048], P('fs'), may hold values from -0.6 to 0.6
- query_cols: float32 [8, 128, 128], P('tp'), may hold values from -0.6 to 0.6
- forget_cols: float32 [8, 128, 128], P('tp'), may hold values from -0.6 to 0.6
- query_row_root: bfloat16 [2048, 2048], P('fs'), may hold values from -2 to 2, as said below
- forget_row_root: bfloat16 [2048, 2048], P('fs'), may hold values from -2 to 2, as said below
- query_col_root: bfloat16 [8, 128, 128], P('tp'), may hold values from -2 to 2, as said below
- forget_col_root: bfloat16 [8, 128, 128], P('tp'), may hold values from -2 to 2, as said below
Outputs:
- query_master: float32 [2048, 1024], P('fs', 'tp')
- forget_master: float32 [2048, 1024], P('fs', 'tp')
- query_copy: bfloat16 [2048, 1024], P('fs', 'tp')
- forget_copy: bfloat16 [2048, 1024], P('fs', 'tp')
- query_step: float32 [2048, 1024], P('fs', 'tp')
- forget_step: float32 [2048, 1024], P('fs', 'tp')
- query_moment_next: float32 [2048, 1024], P('fs', 'tp')
- forget_moment_next: float32 [2048, 1024], P('fs', 'tp')
- query_rows_next: float32 [2048, 2048], P('fs')
- forget_rows_next: float32 [2048, 2048], P('fs')
- query_cols_next: float32 [8, 128, 128], P('tp')
- forget_cols_next: float32 [8, 128, 128], P('tp')
The draws below stay inside these ranges and needn't reach their ends.
Inputs may be any that keep to these rules, and one draw needn't show every extreme that they name: `query_row_root`: diagonal entries 0.5 to 1.5, the others of order 2048 ** -0.5. `forget_row_root`: diagonal entries 0.5 to 1.5, the others of order 2048 ** -0.5. `query_col_root`: diagonal entries 0.5 to 1.5, the others of order 128 ** -0.5. `forget_col_root`: diagonal entries 0.5 to 1.5, the others of order 128 ** -0.5.
All inputs are finite; a program needn't handle non-finite values.
Results may differ from the reference program's by a relative error of at most 0.005.
Values may be sent and summed in bfloat16 or wider, within the bound.
A program may use at most 64 MiB of HBM per device.

```python
import jax
import jax.numpy as jnp
from jax import lax

D = 2048
HW = 1024
HEAD = 128
TOKENS = 16384
HEADS = 8


def root_matrix(key, shape):
    order = shape[-1]
    diag_key, spread_key = jax.random.split(key)
    spread = jnp.clip(jax.random.normal(spread_key, shape, jnp.float32), -4.0, 4.0) * order ** (-0.5)
    diagonal = jax.random.uniform(diag_key, shape[:-1], jnp.float32, 0.5, 1.5)
    unit_eye = jnp.eye(order, dtype=jnp.float32)
    return (spread * (1.0 - unit_eye) + diagonal[..., None] * unit_eye).astype(jnp.bfloat16)


def draw_query_row_root(key, part):
    return root_matrix(jax.random.fold_in(key, 11), (D, D))


def draw_forget_row_root(key, part):
    return root_matrix(jax.random.fold_in(key, 23), (D, D))


def draw_query_col_root(key, part):
    return root_matrix(jax.random.fold_in(key, 37), (HEADS, HEAD, HEAD))


def draw_forget_col_root(key, part):
    return root_matrix(jax.random.fold_in(key, 41), (HEADS, HEAD, HEAD))


def raised(entries, own_key, source, target, parts, factor):
    owner, partner = [(jnp.arange(entries.shape[dim]) // (entries.shape[dim] // parts)).reshape([-1 if axis == dim else 1 for axis in range(entries.ndim)]) for dim in (source, target)]
    chosen = jax.random.permutation(own_key, parts)[partner]
    strong = (owner == chosen) | (owner == (partner + parts // 2) % parts)
    return jnp.where(strong, factor * entries, entries)


def steps_of(rng, shape, shards, low, high):
    factor_of, own = 1.0, jax.random.fold_in(rng, 6)
    for dim, shards_of in shards:
        steps = jnp.exp(jax.random.uniform(jax.random.fold_in(own, dim), (shards_of,), jnp.float32, low / len(shards), high / len(shards)))
        factor_of = factor_of * jnp.repeat(steps, shape[dim] // shards_of).reshape([-1 if axis == dim else 1 for axis in range(len(shape))])
    return factor_of


def gaussian(rng, extent, deviation, bound, cuts=(), kind=jnp.bfloat16):
    array = jax.random.normal(rng, extent, jnp.float32) * deviation
    if len(cuts) > 0:
        array = steps_of(rng, extent, cuts, -0.22, 0.18) * array
    return jnp.clip(array, min=-bound, max=bound).astype(kind)


def bell_draw_with(key, extent, deviation, limit, shards, heavy, held_as=jnp.bfloat16):
    drawn = deviation * jax.random.normal(key, extent, jnp.float32)
    if shards:
        drawn = drawn * steps_of(key, extent, shards, -0.22, 0.18)
    return jnp.clip(raised(drawn, jax.random.fold_in(key, 3), *heavy), -limit, limit).astype(held_as)


def setup_inputs(seed: int = 0) -> dict:
    key_list = jax.random.split(jax.random.key(seed), 18)
    inputs = bell_draw_with(key_list[0], (TOKENS, D), 1.0, 24.0, ((0, 128), (1, 4)), (0, 1, 128, 5.5))
    query_grad = gaussian(key_list[1], (TOKENS, HW), 1.0, 6.0, ((0, 128), (1, 4)))
    forget_grad = gaussian(key_list[2], (TOKENS, HW), 1.0, 6.0, ((0, 128), (1, 4)))
    forget_pre = gaussian(key_list[3], (TOKENS, HW), 2.0, 8.0, ((0, 128), (1, 4)))
    lower_bound = jnp.clip(0.1 + 0.79999997 * jax.random.uniform(key_list[4], (HW,), jnp.float32) ** steps_of(key_list[4], (HW,), ((0, 4),), -0.2, 0.2), 0.1, 0.9)
    query_weight = gaussian(key_list[5], (D, HW), D ** -0.5, 0.125, ((0, 128), (1, 4)), jnp.float32)
    forget_weight = gaussian(key_list[6], (D, HW), D ** -0.5, 0.125, ((0, 128), (1, 4)), jnp.float32)
    query_moment = gaussian(key_list[7], (D, HW), 1.0, 6.0, ((0, 128), (1, 4)), jnp.float32)
    forget_moment = gaussian(key_list[8], (D, HW), 1.0, 6.0, ((0, 128), (1, 4)), jnp.float32)
    query_rows = gaussian(key_list[9], (D, D), 0.1, 0.6, ((0, 128),), jnp.float32)
    forget_rows = gaussian(key_list[10], (D, D), 0.1, 0.6, ((0, 128),), jnp.float32)
    query_cols = gaussian(key_list[11], (HEADS, HEAD, HEAD), 0.1, 0.6, ((0, 4),), jnp.float32)
    forget_cols = gaussian(key_list[12], (HEADS, HEAD, HEAD), 0.1, 0.6, ((0, 4),), jnp.float32)
    query_row_root = draw_query_row_root(jax.random.fold_in(key_list[17], 71), 0)
    forget_row_root = draw_forget_row_root(jax.random.fold_in(key_list[17], 71), 0)
    query_col_root = draw_query_col_root(jax.random.fold_in(key_list[17], 71), 0)
    forget_col_root = draw_forget_col_root(jax.random.fold_in(key_list[17], 71), 0)
    return dict(inputs=inputs, query_grad=query_grad, forget_grad=forget_grad, forget_pre=forget_pre, lower_bound=lower_bound, query_weight=query_weight, forget_weight=forget_weight, query_moment=query_moment, forget_moment=forget_moment, query_rows=query_rows, forget_rows=forget_rows, query_cols=query_cols, forget_cols=forget_cols, query_row_root=query_row_root, forget_row_root=forget_row_root, query_col_root=query_col_root, forget_col_root=forget_col_root)


stat_decay = 0.9
moment_decay = 0.9
learn_rate = 0.02
highest = lax.Precision.HIGHEST

def finish(gradient, weight, moment, rows, cols, row_root, col_root):
    square = jnp.sum(gradient * gradient)
    norm_scale = jnp.sqrt(D * HW / (square + 1.0))
    scaled = gradient * norm_scale
    rows_next = stat_decay * rows + (1.0 - stat_decay) / HW * jnp.dot(scaled, scaled.T, precision=highest)
    by_head = scaled.reshape(D, HEADS, HEAD)
    cols_next = stat_decay * cols + (1.0 - stat_decay) / D * jnp.einsum('rhi,rhj->hij', by_head, by_head, precision=highest)
    left_sum = jnp.dot(row_root.astype(jnp.float32), gradient, precision=highest)
    precond = norm_scale * jnp.einsum('rhi,hij->rhj', left_sum.reshape(D, HEADS, HEAD), col_root.astype(jnp.float32), precision=highest).reshape(D, HW)
    moment_next = moment_decay * moment + (1.0 - moment_decay) * precond
    update_step = moment_decay * moment_next + (1.0 - moment_decay) * precond
    master = weight - learn_rate * update_step
    return (master, master.astype(jnp.bfloat16), update_step, moment_next, rows_next, cols_next)

def reference(inputs, query_grad, forget_grad, forget_pre, lower_bound, query_weight, forget_weight, query_moment, forget_moment, query_rows, forget_rows, query_cols, forget_cols, query_row_root, forget_row_root, query_col_root, forget_col_root):
    sigma_gate = jax.nn.sigmoid(forget_pre.astype(jnp.float32))
    forget_cot = (forget_grad.astype(jnp.float32) * (1.0 - lower_bound) * sigma_gate * (1.0 - sigma_gate)).astype(jnp.bfloat16)
    query_gradient = jnp.dot(inputs.T, query_grad, preferred_element_type=jnp.float32)
    forget_gradient = jnp.dot(inputs.T, forget_cot, preferred_element_type=jnp.float32)
    query_out = finish(query_gradient, query_weight, query_moment, query_rows, query_cols, query_row_root, query_col_root)
    forget_out = finish(forget_gradient, forget_weight, forget_moment, forget_rows, forget_cols, forget_row_root, forget_col_root)
    return (query_out[0], forget_out[0], query_out[1], forget_out[1], query_out[2], forget_out[2], query_out[3], forget_out[3], query_out[4], forget_out[4], query_out[5], forget_out[5])
```

```python
import jax
import jax.numpy as jnp
from jax import lax
from jax.experimental import pallas as pl
from jax.experimental.pallas import tpu as pltpu
from jax.sharding import Mesh
from jax.sharding import PartitionSpec as P

D = 2048
HW = 1024
HEAD = 128
FS = ("fs_0", "fs_1", "fs_2")
MESH = pl.DeviceIdType.MESH
COPIES = 96

stat_decay = 0.9
moment_decay = 0.9
learn_rate = 0.02
highest = lax.Precision.HIGHEST
f32 = jnp.float32
bf16 = jnp.bfloat16


class Net:
    def __init__(self, send, recv):
        self.send, self.recv, self.made = send, recv, []

    def copy(self, src, dst, **where):
        i = len(self.made)
        made = pltpu.make_async_remote_copy(
            src_ref=src,
            dst_ref=dst,
            send_sem=self.send.at[i],
            recv_sem=self.recv.at[i],
            device_id=where,
            device_id_type=MESH,
        )
        made.start()
        self.made.append(made)
        return made


def dot(a, b):
    return jnp.dot(a, b, preferred_element_type=f32)


def kernel(
    x_ref, qg_ref, fg_ref, fp_ref, lb_ref, rq_ref, rf_ref, cq_ref, cf_ref,
    outer_ref, pre_ref, col_ref, sq_ref,
    xy, xx, tr, gx, rall, rp, pmine, pout, pin, gp, r1, sf, sb, r2, g, o, orv, pres, cols,
    send, recv,
):
    z, x, k, y = (lax.axis_index(n) for n in ("fs_0", "fs_1", "fs_2", "tp"))
    ko = 1 - k
    at = lambda v, n, m: lax.rem(v + n + m, m)
    xp, xm, x2 = at(x, 1, 4), at(x, -1, 4), at(x, 2, 4)
    yp, ym, y2 = at(y, 1, 4), at(y, -1, 4), at(y, 2, 4)
    aw, b = z // 4, lax.rem(z, 4)
    bp, bm, b2 = at(b, 1, 4), at(b, -1, 4), at(b, 2, 4)
    zat = lambda n: at(z, n, 16)
    net = Net(send, recv)

    barrier = pltpu.get_barrier_semaphore()
    partners = [dict(fs_2=ko), dict(fs_1=xp), dict(fs_1=xm)]
    partners += [dict(tp=yy, fs_2=kk) for yy in (yp, ym) for kk in (k, ko)]
    partners += [dict(fs_0=zat(n)) for n in (1, -1, 2, -2, 4, -4, 8)]
    for who in partners:
        pl.semaphore_signal(barrier, inc=1, device_id=who, device_id_type=MESH)

    for n in range(4):
        xy[y, n] = x_ref[:, n * 128 : (n + 1) * 128].T
    gx[x, 0] = qg_ref[...]
    gate = jax.nn.sigmoid(fp_ref[...].astype(f32))
    gx[x, 1] = (fg_ref[...].astype(f32) * (1.0 - lb_ref[...]) * gate * (1.0 - gate)).astype(bf16)
    for n in range(16):
        rall[0, n] = rq_ref[:, n * 128 : (n + 1) * 128]
        rall[1, n] = rf_ref[:, n * 128 : (n + 1) * 128]
    pl.semaphore_wait(barrier, len(partners))

    lo, hi = pl.ds(0, 2), pl.ds(2, 2)
    ya_ = net.copy(xy.at[y, lo], xy.at[y, lo], tp=yp)
    yc_ = net.copy(xy.at[y, hi], xy.at[y, hi], tp=ym)
    ga_ = net.copy(gx.at[x, 0], gx.at[x, 0], fs_1=xp)
    gc_ = net.copy(gx.at[x, 1], gx.at[x, 1], fs_1=xm)
    yb_ = net.copy(xy.at[y, hi], xy.at[y, hi], tp=yp)
    yd_ = net.copy(xy.at[y, lo], xy.at[y, lo], tp=ym)
    gb_ = net.copy(gx.at[x, 1], gx.at[x, 1], fs_1=xp)
    gd_ = net.copy(gx.at[x, 0], gx.at[x, 0], fs_1=xm)
    rc_ = net.copy(rall.at[ko], rp, fs_2=ko)

    at_a = (y, ym, yp, y2)
    xs = {}

    def xsend(j):
        a = at_a[j]
        xs[j] = [
            net.copy(xy.at[a, x2], tr.at[j], fs_1=xp if j % 2 == 0 else xm),
            net.copy(xy.at[a, xp], xx.at[x, a], fs_1=xp),
            net.copy(xy.at[a, xm], xx.at[x, a], fs_1=xm),
        ]
        xx[x, a] = xy[a, x]

    def xforward(j):
        a = at_a[j]
        xs[j][0].wait_recv()
        came, to = (xm, xp) if j % 2 == 0 else (xp, xm)
        xs[j].append(net.copy(tr.at[j], xx.at[came, a], fs_1=to))

    xsend(0)
    ya_.wait_recv()
    ye_ = net.copy(xy.at[ym, lo], xy.at[ym, lo], tp=yp)
    yc_.wait_recv()
    yf_ = net.copy(xy.at[yp, hi], xy.at[yp, hi], tp=ym)
    ga_.wait_recv()
    ge_ = net.copy(gx.at[xm, 0], gx.at[xm, 0], fs_1=xp)
    gc_.wait_recv()
    gf_ = net.copy(gx.at[xp, 1], gx.at[xp, 1], fs_1=xm)
    yb_.wait_recv()
    xsend(1)
    yd_.wait_recv()
    xsend(2)
    xforward(0)
    ye_.wait_recv()
    yf_.wait_recv()
    xsend(3)
    xforward(1)
    for c in (gb_, gd_, ge_, gf_):
        c.wait_recv()

    ps, zs = {}, {}

    def product(j):
        a = at_a[j]
        for c in xs[j][1:]:
            c.wait_recv()
        lhs = jnp.concatenate([xx[n, a] for n in range(4)], axis=1)
        pout[a] = dot(lhs, gx[:, ko].reshape(512, 256))
        pmine[a] = dot(lhs, gx[:, k].reshape(512, 256)).reshape(4, 32, 256)
        ps[j] = net.copy(pout.at[a], pin.at[a], fs_2=ko)

    def near(j):
        a = at_a[j]
        ps[j].wait_recv()
        total = pmine[a] + pin[a].reshape(4, 32, 256)
        pmine[a] = total
        gp[a] = total.astype(bf16)
        zs[j] = [
            net.copy(gp.at[a, bp], r1.at[0, a], fs_0=zat(1)),
            net.copy(gp.at[a, bm], r1.at[1, a], fs_0=zat(-1)),
            net.copy(gp.at[a, b2], r1.at[2, a], fs_0=zat(2 if j % 2 == 0 else -2)),
        ]

    product(0)
    xforward(2)
    near(0)
    product(1)
    xforward(3)
    near(1)
    product(2)
    near(2)
    product(3)
    near(3)
    for j in range(4):
        a = at_a[j]
        for c in zs[j]:
            c.wait_recv()
        total = pmine[a, b]
        for n in range(3):
            total = total + r1[n, a].astype(f32)
        sf[a] = total
        sb[a] = total.astype(bf16)
    far = [net.copy(sb.at[at(aw, i, 4)], r2.at[i - 1], fs_0=zat(4 * i)) for i in (2, 1, 3)]
    for c in far:
        c.wait_recv()
    total = sf[aw]
    for n in range(3):
        total = total + r2[n].astype(f32)
    g[aw, x, b] = total.astype(bf16)

    far = [net.copy(g.at[aw, x, b], g.at[aw, x, b], fs_0=zat(4 * i)) for i in (2, 1, 3)]
    for c in far:
        c.wait_recv()
    n1 = net.copy(g.at[:, x, b], g.at[:, x, b], fs_0=zat(1))
    n2 = net.copy(g.at[:, x, b], g.at[:, x, b], fs_0=zat(-1))
    n3 = net.copy(g.at[lo, x, b], g.at[lo, x, b], fs_0=zat(2))
    n4 = net.copy(g.at[hi, x, b], g.at[hi, x, b], fs_0=zat(-2))

    at_c = (b, bm, bp, b2)
    gs = {}

    def gsend(i):
        c = at_c[i]
        gs[i] = [
            net.copy(g.at[:, x, c], g.at[:, x, c], fs_1=xp),
            net.copy(g.at[:, x, c], g.at[:, x, c], fs_1=xm),
        ]

    def gforward(i):
        c = at_c[i]
        n, came, to = (0, xm, xp) if i % 2 == 0 else (1, xp, xm)
        gs[i][n].wait_recv()
        gs[i].append(net.copy(g.at[:, came, c], g.at[:, came, c], fs_1=to))

    gsend(0)
    n1.wait_recv()
    gsend(1)
    n2.wait_recv()
    gsend(2)
    n3.wait_recv()
    n4.wait_recv()
    gsend(3)
    for i in range(4):
        gforward(i)
    for i in range(4):
        gs[i][1 if i % 2 == 0 else 0].wait_recv()
        gs[i][2].wait_recv()

    square = jnp.zeros((8, 256), f32)
    for a in range(4):
        part = g[a].reshape(512, 256).astype(f32)
        square = square + jnp.sum((part * part).reshape(64, 8, 256), axis=0)
    square = jnp.broadcast_to(jnp.sum(square, axis=(0, 1), keepdims=True), (16, 128))
    rest = square - square.astype(bf16).astype(f32)
    top = lax.broadcasted_iota(jnp.int32, (16, 128), 0) < 8
    coded = jnp.where(top, square, rest).astype(bf16)
    o[0, 16] = coded
    o[1, 16] = coded
    mine = g[aw, b, x]
    for a in range(4):
        block = lax.dot_general(
            mine, g[a].reshape(512, 256), (((1,), (1,)), ((), ())), preferred_element_type=f32
        ).astype(bf16)
        for n in range(4):
            piece = block[:, n * 128 : (n + 1) * 128]
            o[0, 4 * a + n] = piece[:16]
            o[1, 4 * a + n] = piece[16:]
    orv[k, y] = o[k]
    h0, h1 = pl.ds(0, 8), pl.ds(8, 9)
    os = {}
    for kk, half in ((k, 0), (ko, 0), (k, 1), (ko, 1)):
        same = kk is k
        for up in (True, False):
            h = h0 if (half == 0) == up else h1
            os[same, up, h is h0] = net.copy(
                o.at[kk, h], orv.at[k, y, h], tp=yp if up else ym, fs_2=kk
            )
    oc_ = net.copy(o.at[ko], orv.at[k, y], fs_2=ko)

    rc_.wait_recv()
    left = jnp.zeros((32, 256), f32)
    gram = jnp.zeros((256, 256), f32)
    for a in range(4):
        part = g[a].reshape(512, 256)
        root = jnp.concatenate(
            [
                jnp.concatenate([rall[k, 4 * a + n] for n in range(4)], axis=1),
                jnp.concatenate([rp[4 * a + n] for n in range(4)], axis=1),
            ],
            axis=0,
        )
        left = left + dot(root, part)
        gram = gram + lax.dot_general(
            part, part, (((0,), (0,)), ((), ())), preferred_element_type=f32
        )
    for h in range(2):
        lanes = slice(h * 128, (h + 1) * 128)
        cols[0, h] = gram[lanes, lanes]
        root = jnp.where(k == 0, cq_ref[h].astype(f32), cf_ref[h].astype(f32)).astype(bf16)
        value = left[:, lanes]
        high = value.astype(bf16)
        low = (value - high.astype(f32)).astype(bf16)
        pre = dot(high, root) + dot(low, root)
        pres[0, :, lanes] = pre[:16]
        pres[1, :, lanes] = pre[16:]

    fw = []
    for same in (True, False):
        m = k if same else ko
        os[same, True, True].wait_recv()
        fw.append(net.copy(orv.at[m, ym, h0], orv.at[m, ym, h0], tp=yp))
        os[same, False, False].wait_recv()
        fw.append(net.copy(orv.at[m, yp, h1], orv.at[m, yp, h1], tp=ym))
    pc_ = net.copy(pres.at[1], pre_ref.at[k], fs_2=ko)
    cc_ = net.copy(cols.at[0], col_ref.at[k], fs_2=ko)
    pre_ref[k] = pres[0]
    col_ref[k] = cols[0]
    for same in (True, False):
        os[same, True, False].wait_recv()
        os[same, False, True].wait_recv()
    for c in (*fw, oc_, pc_, cc_):
        c.wait_recv()
    for m in range(2):
        for n in range(16):
            total = orv[m, 0, n].astype(f32)
            for q in range(1, 4):
                total = total + orv[m, q, n].astype(f32)
            outer_ref[m, :, n * 128 : (n + 1) * 128] = total
        total = orv[m, 0, 16].astype(f32)
        for q in range(1, 4):
            total = total + orv[m, q, 16].astype(f32)
        sq_ref[m] = total[:8] + total[8:]
    for c in net.made:
        c.wait_send()


def exchange(inputs, qg, fg, fp, lb, rq, rf, cq, cf):
    vm = pl.BlockSpec(memory_space=pltpu.VMEM)
    s = lambda shape, kind=bf16: pltpu.VMEM(shape, kind)
    return pl.pallas_call(
        kernel,
        out_shape=(
            jax.ShapeDtypeStruct((2, 16, D), f32),
            jax.ShapeDtypeStruct((2, 16, 256), f32),
            jax.ShapeDtypeStruct((2, 2, HEAD, HEAD), f32),
            jax.ShapeDtypeStruct((2, 8, 128), f32),
        ),
        in_specs=[vm] * 9,
        out_specs=(vm,) * 4,
        scratch_shapes=[
            s((4, 4, 128, 128)),
            s((4, 4, 128, 128)),
            s((4, 128, 128)),
            s((4, 2, 128, 256)),
            s((2, 16, 16, 128)),
            s((16, 16, 128)),
            s((4, 4, 32, 256), f32),
            s((4, 128, 256), f32),
            s((4, 128, 256), f32),
            s((4, 4, 32, 256)),
            s((3, 4, 32, 256)),
            s((4, 32, 256), f32),
            s((4, 32, 256)),
            s((3, 32, 256)),
            s((4, 4, 4, 32, 256)),
            s((2, 17, 16, 128)),
            s((2, 4, 17, 16, 128)),
            s((2, 16, 256), f32),
            s((1, 2, HEAD, HEAD), f32),
            pltpu.SemaphoreType.DMA((COPIES,)),
            pltpu.SemaphoreType.DMA((COPIES,)),
        ],
        compiler_params=pltpu.CompilerParams(collective_id=0, has_side_effects=True),
        name="exchange",
    )(inputs, qg, fg, fp, lb.reshape(1, -1), rq, rf, cq, cf)


def finish(weight, moment, rows, cols, outer, pre, col, square):
    scale = jnp.sqrt(D * HW / (square + 1.0))
    twice = scale * scale
    rows_next = stat_decay * rows + (1.0 - stat_decay) / HW * twice * outer
    cols_next = stat_decay * cols + (1.0 - stat_decay) / D * twice * col
    precond = scale * pre
    moment_next = moment_decay * moment + (1.0 - moment_decay) * precond
    step = moment_decay * moment_next + (1.0 - moment_decay) * precond
    master = weight - learn_rate * step
    return (master, master.astype(bf16), step, moment_next, rows_next, cols_next)


def on_device(inputs, qg, fg, fp, lb, qw, fw, qm, fm, qr, fr, qc, fc, qrr, frr, qcr, fcr):
    outer, pre, col, square = exchange(inputs, qg, fg, fp, lb, qrr, frr, qcr, fcr)
    q = finish(qw, qm, qr, qc, outer[0], pre[0], col[0], square[0, 0, 0])
    f = finish(fw, fm, fr, fc, outer[1], pre[1], col[1], square[1, 0, 0])
    return tuple(v for pair in zip(q, f) for v in pair)


def solution(mesh):
    split = Mesh(mesh.devices.reshape(16, 4, 2, mesh.shape["tp"]), ("fs_0", "fs_1", "fs_2", "tp"))
    both, rows, cols = P(FS, "tp"), P(FS, None), P("tp", None, None)
    return jax.shard_map(
        on_device,
        mesh=split,
        in_specs=(both,) * 4 + (P("tp"),) + (both,) * 4 + (rows,) * 2 + (cols,) * 2 + (rows,) * 2 + (cols,) * 2,
        out_specs=(both,) * 8 + (rows,) * 2 + (cols,) * 2,
        check_vma=False,
    )
```

```python
import jax
import jax.numpy as jnp
from jax import lax
from jax.experimental import pallas as pl
from jax.experimental.pallas import tpu as pltpu
from jax.sharding import Mesh
from jax.sharding import PartitionSpec as P

D = 2048
HW = 1024
HEAD = 128
FS = ("fs_0", "fs_1", "fs_2")
MESH = pl.DeviceIdType.MESH
COPIES = 90
TILES = 827

stat_decay = 0.9
moment_decay = 0.9
learn_rate = 0.02
highest = lax.Precision.HIGHEST
f32 = jnp.float32
bf16 = jnp.bfloat16


class Net:
    def __init__(self, send, recv):
        self.send, self.recv, self.made, self.tiles = send, recv, [], 0

    def copy(self, src, dst, **where):
        made = pltpu.make_async_remote_copy(
            src_ref=src,
            dst_ref=dst,
            send_sem=self.send,
            recv_sem=self.recv.at[len(self.made)],
            device_id=where,
            device_id_type=MESH,
        )
        made.start()
        self.made.append(made)
        size = src.dtype.itemsize
        for n in src.shape:
            size *= n
        assert size % 4096 == 0
        self.tiles += size // 4096
        return made

    def drain(self, room, **where):
        assert (len(self.made), self.tiles) == (COPIES, TILES), (len(self.made), self.tiles)
        pltpu.make_async_remote_copy(
            src_ref=room,
            dst_ref=room,
            send_sem=self.send,
            recv_sem=self.recv.at[0],
            device_id=where,
            device_id_type=MESH,
        ).wait_send()


def dot(a, b):
    return jnp.dot(a, b, preferred_element_type=f32)


def kernel(
    x_hbm, qg_hbm, fg_hbm, fp_hbm, lb_hbm, rq_hbm, rf_hbm, cq_hbm, cf_hbm,
    outer_ref, pre_ref, col_ref,
    x_ref, qg_ref, fg_ref, fp_ref, lb_ref, rq_ref, rf_ref, cq_ref, cf_ref,
    xt, xx, gx, rall, rp, pmine, pout, pin, gp, r1, sf, sb, r2, g, o, orv, prer, colr, pres, cols,
    room, send, recv, loads,
):
    z, x, k, y = (lax.axis_index(n) for n in ("fs_0", "fs_1", "fs_2", "tp"))
    ko = 1 - k
    at = lambda v, n, m: lax.rem(v + n + m, m)
    xp, xm, x2 = at(x, 1, 4), at(x, -1, 4), at(x, 2, 4)
    yp, ym, y2 = at(y, 1, 4), at(y, -1, 4), at(y, 2, 4)
    aw, b = z // 4, lax.rem(z, 4)
    bp, bm, b2 = at(b, 1, 4), at(b, -1, 4), at(b, 2, 4)
    zat = lambda n: at(z, n, 16)
    net = Net(send, recv)

    barrier = pltpu.get_barrier_semaphore()
    partners = [dict(fs_2=ko), dict(fs_1=xp), dict(fs_1=xm), dict(fs_1=x2)]
    partners += [dict(tp=yy, fs_2=kk) for yy in (yp, ym, y2) for kk in (k, ko)]
    partners += [dict(fs_0=zat(n)) for n in (1, -1, 2, -2, 4, -4, 8)]
    for who in partners:
        pl.semaphore_signal(barrier, inc=1, device_id=who, device_id_type=MESH)

    pairs = (
        (x_hbm, x_ref), (qg_hbm, qg_ref), (fg_hbm, fg_ref), (fp_hbm, fp_ref), (lb_hbm, lb_ref),
        (rq_hbm, rq_ref), (rf_hbm, rf_ref), (cq_hbm, cq_ref), (cf_hbm, cf_ref),
    )
    load = [pltpu.make_async_copy(u, v, loads.at[n]) for n, (u, v) in enumerate(pairs)]
    for c in load:
        c.start()
    load[0].wait()
    for n in range(4):
        turned = x_ref[:, n * 128 : (n + 1) * 128].T
        for q in range(4):
            xt[q, n * 32 : (n + 1) * 32] = turned[q * 32 : (q + 1) * 32]
    xx[y, x] = xt[x]
    for c in load[1:5]:
        c.wait()
    gx[x, 0] = qg_ref[...]
    gate = jax.nn.sigmoid(fp_ref[...].astype(f32))
    gx[x, 1] = (fg_ref[...].astype(f32) * (1.0 - lb_ref[...]) * gate * (1.0 - gate)).astype(bf16)
    for c in load[5:]:
        c.wait()
    for n in range(16):
        rall[0, n] = rq_ref[:, n * 128 : (n + 1) * 128]
        rall[1, n] = rf_ref[:, n * 128 : (n + 1) * 128]
    pl.semaphore_wait(barrier, len(partners))

    first = k == 0
    px = (x, xm, xp, x2)
    at_a = (y, ym, yp, y2)
    ys = {}

    def ysend(p):
        ys[p] = [
            net.copy(xx.at[y, px[p]], xx.at[y, px[p]], tp=yp),
            net.copy(xx.at[y, px[p]], xx.at[y, px[p]], tp=ym),
        ]
        if p == 3:
            ys[p].append(net.copy(xx.at[y, px[p]], xx.at[y, px[p]], tp=y2))

    def yforward(p):
        n, came, to = (0, ym, yp) if p % 2 == 0 else (1, yp, ym)
        ys[p][n].wait_recv()
        ys[p].append(net.copy(xx.at[came, px[p]], xx.at[came, px[p]], tp=to))

    xc_ = net.copy(xt.at[x2], xx.at[y, x], fs_1=x2)
    xa_ = net.copy(xt.at[xp], xx.at[y, x], fs_1=xp)
    xb_ = net.copy(xt.at[xm], xx.at[y, x], fs_1=xm)
    ysend(0)
    ga_ = net.copy(gx.at[x, 0], gx.at[x, 0], fs_1=xp)
    gc_ = net.copy(gx.at[x, 1], gx.at[x, 1], fs_1=xm)
    gb_ = net.copy(gx.at[x, 1], gx.at[x, 1], fs_1=xp)
    gd_ = net.copy(gx.at[x, 0], gx.at[x, 0], fs_1=xm)
    rc_ = net.copy(rall.at[ko], rp, fs_2=ko)
    xa_.wait_recv()
    ysend(1)
    xb_.wait_recv()
    ysend(2)
    yforward(0)
    xc_.wait_recv()
    ysend(3)
    ga_.wait_recv()
    ge_ = net.copy(gx.at[xm, 0], gx.at[xm, 0], fs_1=xp)
    gc_.wait_recv()
    gf_ = net.copy(gx.at[xp, 1], gx.at[xp, 1], fs_1=xm)
    yforward(1)
    yforward(2)
    for c in (gb_, gd_, ge_, gf_):
        c.wait_recv()

    ps, zs = {}, {}

    def product(j):
        a = at_a[j]
        lhs = jnp.concatenate([xx[a, n] for n in range(4)], axis=1)
        pout[a] = dot(lhs, gx[:, ko].reshape(512, 256))
        pmine[a] = dot(lhs, gx[:, k].reshape(512, 256)).reshape(4, 32, 256)
        ps[j] = net.copy(pout.at[a], pin.at[a], fs_2=ko)

    def near(j):
        a = at_a[j]
        ps[j].wait_recv()
        total = pmine[a] + pin[a].reshape(4, 32, 256)
        pmine[a] = total
        gp[a] = total.astype(bf16)
        zs[j] = [
            net.copy(gp.at[a, bp], r1.at[0, a], fs_0=zat(1)),
            net.copy(gp.at[a, bm], r1.at[1, a], fs_0=zat(-1)),
            net.copy(gp.at[a, b2], r1.at[2, a], fs_0=zat(2 if j % 2 == 0 else -2)),
        ]

    product(0)
    for p in (1, 3):
        ys[p][0].wait_recv()
    product(1)
    near(0)
    for p in (0, 2, 3):
        ys[p][1].wait_recv()
    product(2)
    near(1)
    for p in range(4):
        ys[p][2].wait_recv()
    product(3)
    near(2)
    near(3)
    for j in range(4):
        a = at_a[j]
        for c in zs[j]:
            c.wait_recv()
        total = pmine[a, b]
        for n in range(3):
            total = total + r1[n, a].astype(f32)
        sf[a] = total
        sb[a] = total.astype(bf16)
    far = [net.copy(sb.at[at(aw, i, 4)], r2.at[i - 1], fs_0=zat(4 * i)) for i in (2, 1, 3)]
    for c in far:
        c.wait_recv()
    total = sf[aw]
    for n in range(3):
        total = total + r2[n].astype(f32)
    mine = total.astype(bf16)
    g[aw, b, x] = mine

    far = [net.copy(g.at[aw, b, x], g.at[aw, b, x], fs_0=zat(4 * i)) for i in (2, 1, 3)]
    rc_.wait_recv()
    for c in far:
        c.wait_recv()
    lo, hi = pl.ds(0, 2), pl.ds(2, 2)
    n1 = net.copy(g.at[:, b, x], g.at[:, b, x], fs_0=zat(1))
    n2 = net.copy(g.at[:, b, x], g.at[:, b, x], fs_0=zat(-1))
    n3 = net.copy(g.at[lo, b, x], g.at[lo, b, x], fs_0=zat(2))
    n4 = net.copy(g.at[hi, b, x], g.at[hi, b, x], fs_0=zat(-2))

    at_c = (b, bm, bp, b2)
    gs, os, fw = {}, {}, []
    state = dict(left=jnp.zeros((32, 256), f32), gram=jnp.zeros((256, 256), f32), square=jnp.zeros((8, 256), f32))

    def gcopy(c, n, **where):
        return net.copy(g.at[:, c, n], g.at[:, c, n], **where)

    def gsend(i):
        gs[i, "up"] = gcopy(at_c[i], x, fs_1=xp) if i != 1 else None
        gs[i, "down"] = gcopy(at_c[i], x, fs_1=xm) if i != 2 else None

    def gforward(i):
        way, came, to = ("up", xm, xp) if i % 2 == 0 else ("down", xp, xm)
        gs[i, way].wait_recv()
        gs[i, "on"] = gcopy(at_c[i], came, fs_1=to)

    def gwait(i):
        if i == 1:
            gs["z", "up"].wait_recv()
        elif i == 2:
            gs["z", "down"].wait_recv()
        elif i == 3:
            gs[i, "up"].wait_recv()
        gs[i, "on"].wait_recv()

    chunk = lambda i: pl.ds(4 * i, 4 if i < 3 else 5)
    held = lambda i: g[:, at_c[i]].reshape(512, 256)

    def outer(i):
        part = held(i)
        wide = part.astype(f32)
        state["square"] = state["square"] + jnp.sum((wide * wide).reshape(64, 8, 256), axis=0)
        block = lax.dot_general(mine, part, (((1,), (1,)), ((), ())), preferred_element_type=f32).astype(bf16)
        for a in range(4):
            piece = block[:, a * 128 : (a + 1) * 128]
            o[0, 4 * i + a] = piece[:16]
            o[1, 4 * i + a] = piece[16:]
        if i == 3:
            square = jnp.sum(state["square"], axis=(0, 1), keepdims=True)
            square = jnp.broadcast_to(square, (16, 128))
            rest = square - square.astype(bf16).astype(f32)
            top = lax.broadcasted_iota(jnp.int32, (16, 128), 0) < 8
            coded = jnp.where(top, square, rest).astype(bf16)
            o[0, 16] = coded
            o[1, 16] = coded
        h = chunk(i)
        orv[k, y, h] = o[k, h]
        for same, kk in ((True, k), (False, ko)):
            if i == 3:
                os[i, same] = net.copy(o.at[kk, h], orv.at[k, y, h], tp=y2, fs_2=kk)
            for up in (True, False) if i % 2 == 0 else (False, True):
                os[i, same, up] = net.copy(o.at[kk, h], orv.at[k, y, h], tp=yp if up else ym, fs_2=kk)
        os[i] = net.copy(o.at[ko, h], orv.at[k, y, h], fs_2=ko)

    def stats(i):
        part, c = held(i), at_c[i]
        root = jnp.concatenate(
            [
                jnp.concatenate([rall[k, 4 * a + c] for a in range(4)], axis=1),
                jnp.concatenate([rp[4 * a + c] for a in range(4)], axis=1),
            ],
            axis=0,
        )
        state["left"] = state["left"] + dot(root, part)
        state["gram"] = state["gram"] + lax.dot_general(
            part, part, (((0,), (0,)), ((), ())), preferred_element_type=f32
        )

    def oforward(i):
        up, came, to = (True, ym, yp) if i % 2 == 0 else (False, yp, ym)
        h = chunk(i)
        for same, m in ((True, k), (False, ko)):
            os[i, same, up].wait_recv()
            fw.append(net.copy(orv.at[m, came, h], orv.at[m, came, h], tp=to))

    gsend(0)
    n1.wait_recv()
    gsend(1)
    n2.wait_recv()
    gsend(2)
    gforward(0)
    gs["z", "up"] = gcopy(b, xm, fs_0=zat(1))
    gs[0, "down"].wait_recv()
    gs["z", "down"] = gcopy(b, xp, fs_0=zat(-1))
    n3.wait_recv()
    n4.wait_recv()
    gsend(3)
    gforward(1)
    gforward(2)
    gwait(0)
    outer(0)
    gforward(3)
    stats(0)
    gwait(1)
    outer(1)
    stats(1)
    gwait(2)
    outer(2)
    stats(2)
    gwait(3)
    outer(3)
    oforward(0)
    oforward(1)
    oforward(2)
    stats(3)
    left, gram = state["left"], state["gram"]
    for h in range(2):
        lanes = slice(h * 128, (h + 1) * 128)
        cols[h] = gram[lanes, lanes]
        root = jnp.where(first, cq_ref[h].astype(f32), cf_ref[h].astype(f32)).astype(bf16)
        value = left[:, lanes]
        high = value.astype(bf16)
        low = (value - high.astype(f32)).astype(bf16)
        pre = dot(high, root) + dot(low, root)
        pres[0, :, lanes] = pre[:16]
        pres[1, :, lanes] = pre[16:]
    pc_ = net.copy(pres.at[1], prer.at[k], fs_2=ko)
    cc_ = net.copy(cols, colr.at[k], fs_2=ko)
    prer[k] = pres[0]
    colr[k] = cols[...]
    for i in range(4):
        for same in (True, False):
            if i == 3:
                os[i, same, False].wait_recv()
                os[i, same].wait_recv()
            os[i, same, i % 2 == 1].wait_recv()
        os[i].wait_recv()
    for c in (pc_, cc_):
        c.wait_recv()
    for c in fw:
        c.wait_recv()
    for m in range(2):
        total = orv[m, 0, 16].astype(f32)
        for q in range(1, 4):
            total = total + orv[m, q, 16].astype(f32)
        square = total[:8] + total[8:]
        scale = jnp.sqrt(D * HW / (square + 1.0))[:1]
        twice = scale * scale
        by_row = (1.0 - stat_decay) / HW * twice
        by_col = (1.0 - stat_decay) / D * twice
        for i in range(4):
            for a in range(4):
                total = orv[m, 0, 4 * i + a].astype(f32)
                for q in range(1, 4):
                    total = total + orv[m, q, 4 * i + a].astype(f32)
                lanes = pl.ds(pl.multiple_of((4 * a + at_c[i]) * 128, 128), 128)
                outer_ref[m, :, lanes] = by_row * total
        for h in range(2):
            lanes = slice(h * 128, (h + 1) * 128)
            pre_ref[m, :, lanes] = scale * prer[m, :, lanes]
            col_ref[m, h] = by_col * colr[m, h]
    net.drain(room, fs_2=ko)


def exchange(inputs, qg, fg, fp, lb, rq, rf, cq, cf):
    vm = pl.BlockSpec(memory_space=pltpu.VMEM)
    hbm = pl.BlockSpec(memory_space=pltpu.HBM)
    s = lambda shape, kind=bf16: pltpu.VMEM(shape, kind)
    given = (inputs, qg, fg, fp, lb.reshape(1, -1), rq, rf, cq, cf)
    return pl.pallas_call(
        kernel,
        out_shape=(
            pltpu.VMEM((2, 16, D), f32),
            pltpu.VMEM((2, 16, 256), f32),
            pltpu.VMEM((2, 2, HEAD, HEAD), f32),
        ),
        in_specs=[hbm] * 9,
        out_specs=(vm,) * 3,
        scratch_shapes=[s(v.shape, v.dtype) for v in given]
        + [
            s((4, 128, 128)),
            s((4, 4, 128, 128)),
            s((4, 2, 128, 256)),
            s((2, 16, 16, 128)),
            s((16, 16, 128)),
            s((4, 4, 32, 256), f32),
            s((4, 128, 256), f32),
            s((4, 128, 256), f32),
            s((4, 4, 32, 256)),
            s((3, 4, 32, 256)),
            s((4, 32, 256), f32),
            s((4, 32, 256)),
            s((3, 32, 256)),
            s((4, 4, 4, 32, 256)),
            s((2, 17, 16, 128)),
            s((2, 4, 17, 16, 128)),
            s((2, 16, 256), f32),
            s((2, 2, HEAD, HEAD), f32),
            s((2, 16, 256), f32),
            s((2, HEAD, HEAD), f32),
            s((TILES, 16, 128)),
            pltpu.SemaphoreType.DMA,
            pltpu.SemaphoreType.DMA((COPIES,)),
            pltpu.SemaphoreType.DMA((len(given),)),
        ],
        compiler_params=pltpu.CompilerParams(collective_id=0, has_side_effects=True),
        name="exchange",
    )(*given)


def finish(weight, moment, rows, cols, outer, precond, col):
    rows_next = stat_decay * rows + outer
    cols_next = stat_decay * cols + col
    moment_next = moment_decay * moment + (1.0 - moment_decay) * precond
    step = moment_decay * moment_next + (1.0 - moment_decay) * precond
    master = weight - learn_rate * step
    return (master, master.astype(bf16), step, moment_next, rows_next, cols_next)


def on_device(inputs, qg, fg, fp, lb, qw, fw, qm, fm, qr, fr, qc, fc, qrr, frr, qcr, fcr):
    outer, pre, col = exchange(inputs, qg, fg, fp, lb, qrr, frr, qcr, fcr)
    q = finish(qw, qm, qr, qc, outer[0], pre[0], col[0])
    f = finish(fw, fm, fr, fc, outer[1], pre[1], col[1])
    return tuple(v for pair in zip(q, f) for v in pair)


def solution(mesh):
    split = Mesh(mesh.devices.reshape(16, 4, 2, mesh.shape["tp"]), ("fs_0", "fs_1", "fs_2", "tp"))
    both, rows, cols = P(FS, "tp"), P(FS, None), P("tp", None, None)
    return jax.shard_map(
        on_device,
        mesh=split,
        in_specs=(both,) * 4 + (P("tp"),) + (both,) * 4 + (rows,) * 2 + (cols,) * 2 + (rows,) * 2 + (cols,) * 2,
        out_specs=(both,) * 8 + (rows,) * 2 + (cols,) * 2,
        check_vma=False,
    )
```

```python
import jax
import jax.numpy as jnp
from jax import lax
from jax.experimental import pallas as pl
from jax.experimental.pallas import tpu as pltpu
from jax.sharding import Mesh
from jax.sharding import PartitionSpec as P

D = 2048
HW = 1024
HEAD = 128
FS = ("fs_0", "fs_1", "fs_2")
MESH = pl.DeviceIdType.MESH
SEMS = 26
TILES = 746

stat_decay = 0.9
moment_decay = 0.9
learn_rate = 0.02
highest = lax.Precision.HIGHEST
f32 = jnp.float32
bf16 = jnp.bfloat16


class Net:
    def __init__(self, send, recv, room, other):
        self.send, self.recv, self.room, self.other = send, recv, room, other
        self.names, self.sent, self.waited = {}, {}, {}

    def sem(self, name):
        return self.recv.at[self.names.setdefault(name, len(self.names))]

    def copy(self, name, src, dst, count=True, **where):
        pltpu.make_async_remote_copy(
            src_ref=src,
            dst_ref=dst,
            send_sem=self.send,
            recv_sem=self.sem(name),
            device_id=where,
            device_id_type=MESH,
        ).start()
        size = src.dtype.itemsize
        for n in src.shape:
            size *= n
        assert size % 4096 == 0
        if count:
            self.sent[name] = self.sent.get(name, 0) + size // 4096

    def tiles(self, sem, tiles):
        room = self.room.at[pl.ds(0, tiles)]
        return pltpu.make_async_remote_copy(
            src_ref=room,
            dst_ref=room,
            send_sem=self.send,
            recv_sem=sem,
            device_id=self.other,
            device_id_type=MESH,
        )

    def wait(self, name):
        assert name not in self.waited
        self.waited[name] = self.sent[name]
        self.tiles(self.sem(name), self.sent[name]).wait_recv()

    def drain(self):
        assert self.waited == self.sent
        total = sum(self.sent.values())
        assert (len(self.names), total) == (SEMS, TILES), (len(self.names), total)
        self.tiles(self.recv.at[0], total).wait_send()


def dot(a, b):
    return jnp.dot(a, b, preferred_element_type=f32)


def kernel(
    x_hbm, qg_hbm, fg_hbm, fp_hbm, lb_hbm, rq_hbm, rf_hbm, cq_hbm, cf_hbm,
    outer_ref, pre_ref, col_ref,
    x_ref, qg_ref, fg_ref, fp_ref, lb_ref, rq_ref, rf_ref, cq_ref, cf_ref,
    xt, xx, gx, rpack, rin, pmine, pout, pin, gp, rd, ru, sb, rf, gz, gc, o, orv, lp, lin, gram, gin, col, colin, sq, sqx, sqy,
    room, send, recv, loads,
):
    z, x, k, y = (lax.axis_index(n) for n in ("fs_0", "fs_1", "fs_2", "tp"))
    ko = 1 - k
    at = lambda v, n, m: lax.rem(v + n + m, m)
    ym, yp, y2 = at(y, -1, 4), at(y, 1, 4), at(y, 2, 4)
    zat = lambda n: at(z, n, 16)
    net = Net(send, recv, room, dict(fs_2=ko))
    steps = (2, 1, 3)
    plane = [
        (dx, dy, kk)
        for dx, dy in ((2, 2), (1, 2), (3, 2), (2, 1), (2, 3), (1, 1), (3, 3), (1, 3), (3, 1), (2, 0), (0, 2), (1, 0), (0, 1), (3, 0), (0, 3), (0, 0))
        for kk in (k, ko)
        if (dx, dy) != (0, 0) or kk is ko
    ]

    barrier = pltpu.get_barrier_semaphore()
    partners = [dict(fs_1=at(x, dx, 4), tp=at(y, dy, 4), fs_2=kk) for dx, dy, kk in plane]
    partners += [dict(fs_0=zat(n)) for n in (6, -6, 3, -3, 2, -2, 1, -1)]
    for who in partners:
        pl.semaphore_signal(barrier, inc=1, device_id=who, device_id_type=MESH)

    pairs = (
        (x_hbm, x_ref), (qg_hbm, qg_ref), (fg_hbm, fg_ref), (fp_hbm, fp_ref), (lb_hbm, lb_ref),
        (rq_hbm, rq_ref), (rf_hbm, rf_ref), (cq_hbm, cq_ref), (cf_hbm, cf_ref),
    )
    load = [pltpu.make_async_copy(u, v, loads.at[n]) for n, (u, v) in enumerate(pairs)]
    for c in load:
        c.start()
    load[0].wait()
    for n in range(4):
        turned = x_ref[:, n * 128 : (n + 1) * 128].T
        for q in range(4):
            xt[q, n * 32 : (n + 1) * 32] = turned[q * 32 : (q + 1) * 32]
    xx[y, x] = xt[x]
    for c in load[1:5]:
        c.wait()
    gx[x, 0] = qg_ref[...]
    gate = jax.nn.sigmoid(fp_ref[...].astype(f32))
    gx[x, 1] = (fg_ref[...].astype(f32) * (1.0 - lb_ref[...]) * gate * (1.0 - gate)).astype(bf16)
    for c in load[5:]:
        c.wait()
    for m, ref in enumerate((rq_ref, rf_ref)):
        for n in range(4):
            wide = ref[:, n * 512 : (n + 1) * 512].astype(f32)
            for q in range(4):
                strips = [wide[:, w * 128 + q * 32 : w * 128 + (q + 1) * 32] for w in range(4)]
                rpack[m, q, n] = jnp.concatenate(strips, axis=1).astype(bf16)
    rin[x, k] = rpack[k, x]
    pl.semaphore_wait(barrier, len(partners))

    for d in steps:
        net.copy(("x", d), xt.at[at(x, d, 4)], xx.at[y, x], fs_1=at(x, d, 4))

    def ysend(n):
        for d in steps:
            net.copy(("y", d), xx.at[y, n], xx.at[y, n], tp=at(y, d, 4))

    ysend(x)
    for d in steps:
        net.copy("g", gx.at[x], gx.at[x], fs_1=at(x, d, 4))
    net.copy("r", rpack.at[ko, x], rin.at[x, k], fs_2=ko)
    for d in (1, 3, 2):
        net.wait(("x", d))
        ysend(at(x, -d, 4))

    def product(j, a):
        lhs = jnp.concatenate([xx[a, n] for n in range(4)], axis=1)
        pout[a] = dot(lhs, gx[:, ko].reshape(512, 256))
        pmine[a] = dot(lhs, gx[:, k].reshape(512, 256)).reshape(4, 32, 256)
        net.copy(("p", j), pout.at[a], pin.at[a], fs_2=ko)

    def scatter(j, a):
        net.wait(("p", j))
        total = pmine[a] + pin[a].reshape(4, 32, 256)
        pmine[a] = total
        gp[a] = total.astype(bf16)
        for q in range(4):
            t = 4 * a + q
            d = at(t, -z, 16)
            up = (d == 4) | (d == 5) | (d == 7) | (d == 8)
            down = (d == 9) | (d == 11) | (d == 12)
            direct = (d == 1) | (d == 2) | (d == 3) | (d == 13) | (d == 14) | (d == 15)

            @pl.when(up | down)
            def _():
                slot = d - jnp.where(up, 4, 3)
                relay = lax.rem(t + jnp.where(up, 10, 6), 16)
                net.copy("u", gp.at[a, q], ru.at[slot], count=False, fs_0=relay)

            @pl.when(direct)
            def _():
                net.copy("s", gp.at[a, q], rd.at[lax.rem(d + 3, 16)], count=False, fs_0=t)

    net.wait("g")
    product(0, y)
    net.wait(("y", 1))
    product(1, ym)
    net.wait(("y", 3))
    product(2, yp)
    scatter(0, y)
    net.wait(("y", 2))
    product(3, y2)
    scatter(1, ym)
    scatter(2, yp)
    scatter(3, y2)
    for dx in steps:
        for m, kk in ((k, k), (ko, ko)):
            net.copy("r", rpack.at[m, at(x, dx, 4)], rin.at[x, k], fs_1=at(x, dx, 4), fs_2=kk)
    net.sent["s"], net.sent["u"] = 6 * 4, 7 * 4
    net.wait("u")
    part = lambda t: pmine[t // 4, lax.rem(t, 4)]
    for n, to, slots in ((0, zat(6), (0, 1, 3, 4)), (1, zat(-6), (6, 8, 9))):
        total = part(to)
        for i in slots:
            total = total + ru[i].astype(f32)
        sb[n] = total.astype(bf16)
        net.copy("f", sb.at[n], rf.at[n], fs_0=to)
    net.wait("s")
    total = part(z)
    for i in (0, 1, 2, 4, 5, 6):
        total = total + rd[i].astype(f32)
    net.wait("f")
    total = total + rf[0].astype(f32) + rf[1].astype(f32)
    mine = total.astype(bf16)
    gc[z] = mine
    gz[x] = mine

    chunks = ((0, 1, -1, 2), (-2, 3, -3, 6), (-6, -7, -5, 5), (7, -8, -4, 4))

    def zsend(name, e, n):
        net.copy(("z", name), gc.at[zat(e)], gc.at[zat(e)], fs_0=zat(n))

    for n in (6, -6):
        zsend(-n, 0, n)
    for n in (3, -3, 2, -2, 1, -1):
        zsend("direct", 0, n)
    for d in steps:
        net.copy("gz", gz.at[x], gz.at[x], fs_1=at(x, d, 4))
    net.wait("r")
    net.wait(("z", 6))
    for n in (2, 1, -1):
        zsend("relay", 6, n)
    net.wait(("z", -6))
    for n in (2, -2, 1, -1):
        zsend("relay", -6, n)
    net.wait(("z", "direct"))
    net.wait("gz")
    rows = gz[...].reshape(128, 256)

    def outer(i):
        cols = jnp.concatenate([gc[zat(e)] for e in chunks[i]], axis=0)
        block = lax.dot_general(rows, cols, (((1,), (1,)), ((), ())), preferred_element_type=f32).astype(bf16)
        for q in range(8):
            o[q // 2, q % 2, i] = block[q * 16 : (q + 1) * 16]

    def osend(h):
        orv[k, x, y, h] = o[x, k, h]
        for dx, dy, kk in plane:
            to_x, to_y = at(x, dx, 4), at(y, dy, 4)
            net.copy("o", o.at[to_x, kk, h], orv.at[k, x, y, h], fs_1=to_x, tp=to_y, fs_2=kk)

    outer(0)
    outer(1)
    osend(pl.ds(0, 2))
    net.wait(("z", "relay"))
    whole = gc[...].reshape(512, 256)
    wide = whole.astype(f32)
    square = jnp.sum((wide * wide).reshape(64, 8, 256), axis=0)
    sq[...] = jnp.broadcast_to(jnp.sum(square, axis=(0, 1), keepdims=True), (8, 128))
    sqx[x] = sq[...]
    for h in range(2):
        lanes = slice(h * 128, (h + 1) * 128)
        turned = whole[:, lanes]
        gram[h] = lax.dot_general(turned, turned, (((0,), (0,)), ((), ())), preferred_element_type=f32).astype(bf16)
    for d in steps:
        net.copy("q", sq, sqx.at[x], fs_1=at(x, d, 4))
        net.copy("gram", gram, gin.at[x], fs_1=at(x, d, 4))
    outer(2)
    outer(3)
    osend(pl.ds(2, 2))
    roots = rin[...].reshape(8, 4, 16, 128)
    roots = jnp.concatenate(
        [jnp.concatenate([roots[q, n] for n in range(4)], axis=1) for q in range(8)], axis=0
    )
    left = dot(roots, whole)
    lp[...] = left.reshape(4, 2, 16, 256)
    lin[k, x] = lp[x, k]
    for dx in (2, 1, 3, 0):
        for kk in (k, ko):
            if dx or kk is ko:
                to_x = at(x, dx, 4)
                net.copy("l", lp.at[to_x, kk], lin.at[k, x], fs_1=to_x, fs_2=kk)
    net.wait("q")
    total = sqx[0] + sqx[1] + sqx[2] + sqx[3]
    sq2 = sqy.at[k, y]
    sq2[...] = total
    for d in steps:
        for kk in (k, ko):
            net.copy("sqy", sqy.at[k, y], sqy.at[k, y], tp=at(y, d, 4), fs_2=kk)
    net.copy("sqy", sqy.at[k, y], sqy.at[k, y], fs_2=ko)
    net.wait("gram")
    gin[x] = gram[...]
    col[...] = gin[0].astype(f32) + gin[1].astype(f32) + gin[2].astype(f32) + gin[3].astype(f32)
    net.copy("col", col, colin.at[k], fs_2=ko)
    colin[k] = col[...]
    net.wait("l")
    pre = {}
    for m, ref in enumerate((cq_ref, cf_ref)):
        value = lin[m, 0] + lin[m, 1] + lin[m, 2] + lin[m, 3]
        high = value.astype(bf16)
        low = (value - high.astype(f32)).astype(bf16)
        for h in range(2):
            lanes = slice(h * 128, (h + 1) * 128)
            pre[m, h] = dot(high[:, lanes], ref[h]) + dot(low[:, lanes], ref[h])
    net.wait("o")
    net.wait("col")
    net.wait("sqy")
    lane = lax.broadcasted_iota(jnp.int32, (16, 128), 1) // 32
    for m in range(2):
        square = sqy[m, 0] + sqy[m, 1] + sqy[m, 2] + sqy[m, 3]
        scale = jnp.sqrt(D * HW / (square + 1.0))[:1]
        twice = scale * scale
        by_row = (1.0 - stat_decay) / HW * twice
        by_col = (1.0 - stat_decay) / D * twice
        for i in range(4):
            sums = []
            for n in range(4):
                total = orv[m, n, 0, i].astype(f32)
                for q in range(1, 4):
                    total = total + orv[m, n, q, i].astype(f32)
                sums.append(by_row * total)
            for e in range(4):
                block = sums[0] if e == 0 else pltpu.roll(sums[0], (128 - 32 * e) % 128, 1)
                for n in range(1, 4):
                    turn = (32 * (n - e)) % 128
                    block = jnp.where(lane == n, pltpu.roll(sums[n], turn, 1) if turn else sums[n], block)
                lanes = pl.ds(pl.multiple_of(zat(chunks[i][e]) * 128, 128), 128)
                outer_ref[m, :, lanes] = block
        for h in range(2):
            lanes = slice(h * 128, (h + 1) * 128)
            pre_ref[m, :, lanes] = scale * pre[m, h]
            col_ref[m, h] = by_col * colin[m, h]
    net.drain()


def exchange(inputs, qg, fg, fp, lb, rq, rf, cq, cf):
    vm = pl.BlockSpec(memory_space=pltpu.VMEM)
    hbm = pl.BlockSpec(memory_space=pltpu.HBM)
    s = lambda shape, kind=bf16: pltpu.VMEM(shape, kind)
    given = (inputs, qg, fg, fp, lb.reshape(1, -1), rq, rf, cq, cf)
    return pl.pallas_call(
        kernel,
        out_shape=(
            pltpu.VMEM((2, 16, D), f32),
            pltpu.VMEM((2, 16, 256), f32),
            pltpu.VMEM((2, 2, HEAD, HEAD), f32),
        ),
        in_specs=[hbm] * 9,
        out_specs=(vm,) * 3,
        scratch_shapes=[s(v.shape, v.dtype) for v in given]
        + [
            s((4, 128, 128)),
            s((4, 4, 128, 128)),
            s((4, 2, 128, 256)),
            s((2, 4, 4, 16, 128)),
            s((4, 2, 4, 16, 128)),
            s((4, 4, 32, 256), f32),
            s((4, 128, 256), f32),
            s((4, 128, 256), f32),
            s((4, 4, 32, 256)),
            s((7, 32, 256)),
            s((10, 32, 256)),
            s((2, 32, 256)),
            s((2, 32, 256)),
            s((4, 32, 256)),
            s((16, 32, 256)),
            s((4, 2, 4, 16, 128)),
            s((2, 4, 4, 4, 16, 128)),
            s((4, 2, 16, 256), f32),
            s((2, 4, 16, 256), f32),
            s((2, HEAD, HEAD)),
            s((4, 2, HEAD, HEAD)),
            s((2, HEAD, HEAD), f32),
            s((2, 2, HEAD, HEAD), f32),
            s((8, 128), f32),
            s((4, 8, 128), f32),
            s((2, 4, 8, 128), f32),
            s((TILES, 16, 128)),
            pltpu.SemaphoreType.DMA,
            pltpu.SemaphoreType.DMA((SEMS,)),
            pltpu.SemaphoreType.DMA((len(given),)),
        ],
        compiler_params=pltpu.CompilerParams(collective_id=0, has_side_effects=True),
        name="exchange",
    )(*given)


def finish(weight, moment, rows, cols, outer, precond, col):
    rows_next = stat_decay * rows + outer
    cols_next = stat_decay * cols + col
    moment_next = moment_decay * moment + (1.0 - moment_decay) * precond
    step = moment_decay * moment_next + (1.0 - moment_decay) * precond
    master = weight - learn_rate * step
    return (master, master.astype(bf16), step, moment_next, rows_next, cols_next)


def on_device(inputs, qg, fg, fp, lb, qw, fw, qm, fm, qr, fr, qc, fc, qrr, frr, qcr, fcr):
    outer, pre, col = exchange(inputs, qg, fg, fp, lb, qrr, frr, qcr, fcr)
    q = finish(qw, qm, qr, qc, outer[0], pre[0], col[0])
    f = finish(fw, fm, fr, fc, outer[1], pre[1], col[1])
    return tuple(v for pair in zip(q, f) for v in pair)


def solution(mesh):
    split = Mesh(mesh.devices.reshape(16, 4, 2, mesh.shape["tp"]), ("fs_0", "fs_1", "fs_2", "tp"))
    both, rows, cols = P(FS, "tp"), P(FS, None), P("tp", None, None)
    return jax.shard_map(
        on_device,
        mesh=split,
        in_specs=(both,) * 4 + (P("tp"),) + (both,) * 4 + (rows,) * 2 + (cols,) * 2 + (rows,) * 2 + (cols,) * 2,
        out_specs=(both,) * 8 + (rows,) * 2 + (cols,) * 2,
        check_vma=False,
    )
```

```python
import jax
import jax.numpy as jnp
from jax import lax
from jax.experimental import pallas as pl
from jax.experimental.pallas import tpu as pltpu
from jax.sharding import Mesh
from jax.sharding import PartitionSpec as P

D = 2048
HW = 1024
HEAD = 128
FS = ("fs_0", "fs_1", "fs_2")
MESH = pl.DeviceIdType.MESH
SEMS = 22
TILES = 698

stat_decay = 0.9
moment_decay = 0.9
learn_rate = 0.02
highest = lax.Precision.HIGHEST
f32 = jnp.float32
bf16 = jnp.bfloat16


class Net:
    def __init__(self, send, recv, room, other):
        self.send, self.recv, self.room, self.other = send, recv, room, other
        self.names, self.sent, self.waited = {}, {}, {}

    def sem(self, name):
        return self.recv.at[self.names.setdefault(name, len(self.names))]

    def copy(self, name, src, dst, count=True, **where):
        pltpu.make_async_remote_copy(
            src_ref=src,
            dst_ref=dst,
            send_sem=self.send,
            recv_sem=self.sem(name),
            device_id=where,
            device_id_type=MESH,
        ).start()
        size = src.dtype.itemsize
        for n in src.shape:
            size *= n
        assert size % 4096 == 0
        if count:
            self.sent[name] = self.sent.get(name, 0) + size // 4096

    def tiles(self, sem, tiles):
        room = self.room.at[pl.ds(0, tiles)]
        return pltpu.make_async_remote_copy(
            src_ref=room,
            dst_ref=room,
            send_sem=self.send,
            recv_sem=sem,
            device_id=self.other,
            device_id_type=MESH,
        )

    def wait(self, name):
        assert name not in self.waited
        self.waited[name] = self.sent[name]
        self.tiles(self.sem(name), self.sent[name]).wait_recv()

    def drain(self):
        assert self.waited == self.sent
        total = sum(self.sent.values())
        assert (len(self.names), total) == (SEMS, TILES), (len(self.names), total)
        self.tiles(self.recv.at[0], total).wait_send()


def dot(a, b):
    return jnp.dot(a, b, preferred_element_type=f32)


def kernel(
    *refs,
):
    given, refs = refs[:17], refs[17:]
    made, refs = refs[:12], refs[12:]
    held, refs = refs[:17], refs[17:]
    x_ref, qg_ref, fg_ref, fp_ref, lb_ref, rq_ref, rf_ref, cq_ref, cf_ref = held[:9]
    (
    xt, xx, gx, rpack, rin, pmine, pout, pin, gp, rd, ru, sb, rf, gz, gc, o, orv, lp, lin, gram, gin, quarter, colin, sq, sqx, sqsem,
    room, send, recv, loads,
    ) = refs
    z, x, k, y = (lax.axis_index(n) for n in ("fs_0", "fs_1", "fs_2", "tp"))
    ko, b = 1 - k, lax.rem(z, 2)
    at = lambda v, n, m: lax.rem(v + n + m, m)
    ym, yp, y2 = at(y, -1, 4), at(y, 1, 4), at(y, 2, 4)
    zat = lambda n: at(z, n, 16)
    net = Net(send, recv, room, dict(fs_2=ko))
    steps = (2, 1, 3)
    plane = [
        (dx, dy, kk)
        for dx, dy in ((2, 2), (1, 2), (3, 2), (2, 1), (2, 3), (1, 1), (3, 3), (1, 3), (3, 1), (2, 0), (0, 2), (1, 0), (0, 1), (3, 0), (0, 3), (0, 0))
        for kk in (k, ko)
        if (dx, dy) != (0, 0) or kk is ko
    ]

    barrier = pltpu.get_barrier_semaphore()
    partners = [dict(fs_1=at(x, dx, 4), tp=at(y, dy, 4), fs_2=kk) for dx, dy, kk in plane]
    partners += [dict(fs_0=zat(n)) for n in (6, -6, 4, -4, 3, -3, 2, -2, 1, -1)]
    partners += [dict(fs_0=zat(n), fs_2=ko) for n in (1, -1)]
    for who in partners:
        pl.semaphore_signal(barrier, inc=1, device_id=who, device_id_type=MESH)

    load = [pltpu.make_async_copy(u, v, loads.at[n]) for n, (u, v) in enumerate(zip(given, held))]
    for c in load:
        c.start()
    load[0].wait()
    for n in range(4):
        turned = x_ref[:, n * 128 : (n + 1) * 128].T
        for q in range(4):
            xt[q, n * 32 : (n + 1) * 32] = turned[q * 32 : (q + 1) * 32]
    xx[y, x] = xt[x]
    for c in load[1:5]:
        c.wait()
    gx[x, 0] = qg_ref[...]
    gate = jax.nn.sigmoid(fp_ref[...].astype(f32))
    gx[x, 1] = (fg_ref[...].astype(f32) * (1.0 - lb_ref[...]) * gate * (1.0 - gate)).astype(bf16)
    pl.semaphore_wait(barrier, len(partners))

    for d in steps:
        net.copy(("x", d), xt.at[at(x, d, 4)], xx.at[y, x], fs_1=at(x, d, 4))

    def ysend(n):
        for d in steps:
            net.copy(("y", d), xx.at[y, n], xx.at[y, n], tp=at(y, d, 4))

    ysend(x)
    for d in steps:
        net.copy("g", gx.at[x], gx.at[x], fs_1=at(x, d, 4))
    for c in load[5:9]:
        c.wait()
    for m, ref in enumerate((rq_ref, rf_ref)):
        for n in range(4):
            wide = ref[:, n * 512 : (n + 1) * 512].astype(f32)
            for q in range(4):
                strips = [wide[:, w * 128 + q * 32 : w * 128 + (q + 1) * 32] for w in range(4)]
                rpack[m, q, n] = jnp.concatenate(strips, axis=1).astype(bf16)
    rin[x, k] = rpack[k, x]
    net.copy("r", rpack.at[ko, x], rin.at[x, k], fs_2=ko)
    for d in (1, 3, 2):
        net.wait(("x", d))
        ysend(at(x, -d, 4))

    def product(j, a):
        lhs = jnp.concatenate([xx[a, n] for n in range(4)], axis=1)
        pout[a] = dot(lhs, gx[:, ko].reshape(512, 256))
        pmine[a] = dot(lhs, gx[:, k].reshape(512, 256)).reshape(4, 32, 256)
        net.copy(("p", j), pout.at[a], pin.at[a], fs_2=ko)

    def scatter(j, a):
        net.wait(("p", j))
        total = pmine[a] + pin[a].reshape(4, 32, 256)
        pmine[a] = total
        gp[a] = total.astype(bf16)
        for q in range(4):
            t = 4 * a + q
            d = at(t, -z, 16)
            up = (d == 4) | (d == 5) | (d == 7) | (d == 8)
            down = (d == 9) | (d == 11) | (d == 12)
            direct = (d == 1) | (d == 2) | (d == 3) | (d == 13) | (d == 14) | (d == 15)

            @pl.when(up | down)
            def _():
                slot = d - jnp.where(up, 4, 3)
                relay = lax.rem(t + jnp.where(up, 10, 6), 16)
                net.copy("u", gp.at[a, q], ru.at[slot], count=False, fs_0=relay)

            @pl.when(direct)
            def _():
                net.copy("s", gp.at[a, q], rd.at[lax.rem(d + 3, 16)], count=False, fs_0=t)

    net.wait("g")
    product(0, y)
    net.wait(("y", 1))
    product(1, ym)
    net.wait(("y", 3))
    product(2, yp)
    scatter(0, y)
    net.wait(("y", 2))
    product(3, y2)
    scatter(1, ym)
    scatter(2, yp)
    scatter(3, y2)
    for dx in steps:
        for m, kk in ((k, k), (ko, ko)):
            net.copy("r", rpack.at[m, at(x, dx, 4)], rin.at[x, k], fs_1=at(x, dx, 4), fs_2=kk)
    net.sent["s"], net.sent["u"] = 6 * 4, 7 * 4
    net.wait("u")
    part = lambda t: pmine[t // 4, lax.rem(t, 4)]
    for n, e, slots in ((0, 6, (0, 1, 3, 4)), (1, -6, (6, 8, 9))):
        total = part(zat(e))
        for i in slots:
            total = total + ru[i].astype(f32)
        sb[n] = total.astype(bf16)
        net.copy("f", sb.at[n], rf.at[2 + 2 * n], fs_0=zat(e))
        net.copy("f", sb.at[n], rf.at[3 + 2 * n], fs_0=zat(2 * e))
    net.wait("s")
    total = part(z)
    for i in (0, 1, 2, 4, 5, 6):
        total = total + rd[i].astype(f32)
    sb[2] = total.astype(bf16)
    net.copy("f", sb.at[2], rf.at[0], fs_0=zat(6))
    net.copy("f", sb.at[2], rf.at[1], fs_0=zat(-6))
    net.wait("f")

    def joined(mid, above, below):
        return (mid.astype(f32) + above.astype(f32) + below.astype(f32)).astype(bf16)

    mine = joined(sb[2], rf[4], rf[2])
    gc[z] = mine
    gz[x] = mine
    gc[zat(6)] = joined(rf[1], rf[5], sb[0])
    gc[zat(-6)] = joined(rf[0], sb[1], rf[3])

    chunks = ((0, 6, -6, 1), (7, -5, -1, 5), (-7, 2, -8, -4), (-2, 4, 3, -3))
    for d in steps:
        net.copy("gz", gz.at[x], gz.at[x], fs_1=at(x, d, 4))
    for name, n, held_here in (
        ("first", 1, (0, 6, -6)), ("first", -1, (0, 6, -6)), ("last", 3, (0,)), ("last", -3, (0,)),
        ("last", 2, (0, 6, -6)), ("last", -2, (0, -6)),
    ):
        for e in held_here:
            net.copy(("z", name), gc.at[zat(e)], gc.at[zat(e)], fs_0=zat(n))
    net.wait("r")
    net.wait(("z", "first"))
    net.wait("gz")
    rows = gz[...].reshape(128, 256)

    def outer(i):
        cols = jnp.concatenate([gc[zat(e)] for e in chunks[i]], axis=0)
        block = lax.dot_general(rows, cols, (((1,), (1,)), ((), ())), preferred_element_type=f32).astype(bf16)
        for q in range(8):
            o[q // 2, q % 2, i] = block[q * 16 : (q + 1) * 16]

    def osend(h):
        orv[k, x, y, h] = o[x, k, h]
        for dx, dy, kk in plane:
            to_x, to_y = at(x, dx, 4), at(y, dy, 4)
            net.copy("o", o.at[to_x, kk, h], orv.at[k, x, y, h], fs_1=to_x, tp=to_y, fs_2=kk)

    outer(0)
    outer(1)
    osend(pl.ds(0, 2))
    net.wait(("z", "last"))
    whole = gc[...].reshape(512, 256)
    for h in range(2):
        lanes = slice(h * 128, (h + 1) * 128)
        turned = whole[:, lanes]
        both = lax.dot_general(turned, turned, (((0,), (0,)), ((), ())), preferred_element_type=f32).astype(bf16)
        gram[h, 0] = both[:64]
        gram[h, 1] = both[64:]
    for d in steps:
        net.copy("gram", gram.at[b], gin.at[x], fs_1=at(x, d, 4))
    wide = whole.astype(f32)
    square = jnp.sum((wide * wide).reshape(64, 8, 256), axis=0)
    square = jnp.sum(square, axis=(0, 1), keepdims=True)
    sq[0] = jnp.broadcast_to(square, (1, 128))
    outer(2)
    outer(3)
    for n, (dx, dy, kk) in enumerate(plane):
        pltpu.make_async_remote_copy(
            src_ref=sq.at[0],
            dst_ref=sqx.at[n],
            send_sem=sqsem.at[0],
            recv_sem=sqsem.at[1],
            device_id=dict(fs_1=at(x, dx, 4), tp=at(y, dy, 4), fs_2=kk),
            device_id_type=MESH,
        ).start()
    osend(pl.ds(2, 2))
    roots = rin[...].reshape(8, 4, 16, 128)
    roots = jnp.concatenate(
        [jnp.concatenate([roots[q, n] for n in range(4)], axis=1) for q in range(8)], axis=0
    )
    left = dot(roots, whole)
    lp[...] = left.reshape(4, 2, 16, 256).astype(bf16)
    lin[k, x] = lp[x, k]
    for dx in (2, 1, 3, 0):
        for kk in (k, ko):
            if dx or kk is ko:
                to_x = at(x, dx, 4)
                net.copy("l", lp.at[to_x, kk], lin.at[k, x], fs_1=to_x, fs_2=kk)
    net.wait("gram")
    gin[x] = gram[b]
    total = gin[0].astype(f32) + gin[1].astype(f32) + gin[2].astype(f32) + gin[3].astype(f32)
    quarter[...] = total.astype(bf16)
    for n, e in ((0, 1), (1, -1)):
        for kk in (k, ko):
            net.copy("col", quarter.at[n], colin.at[k, b, n], fs_0=zat(e), fs_2=kk)
    net.copy("col", quarter, colin.at[k, b], fs_2=ko)
    colin[k, b] = quarter[...]
    net.wait("l")
    pre = {}
    for m, ref in enumerate((cq_ref, cf_ref)):
        value = lin[m, 0].astype(f32)
        for n in range(1, 4):
            value = value + lin[m, n].astype(f32)
        high = value.astype(bf16)
        low = (value - high.astype(f32)).astype(bf16)
        for h in range(2):
            lanes = slice(h * 128, (h + 1) * 128)
            pre[m, h] = dot(high[:, lanes], ref[h]) + dot(low[:, lanes], ref[h])
    for c in load[9:]:
        c.wait()
    net.wait("o")
    net.wait("col")
    squares = pltpu.make_async_remote_copy(
        src_ref=sqx,
        dst_ref=sqx,
        send_sem=sqsem.at[0],
        recv_sem=sqsem.at[1],
        device_id=dict(fs_2=ko),
        device_id_type=MESH,
    )
    squares.wait_recv()
    squares.wait_send()
    same, cross = sq[0], jnp.zeros((1, 128), f32)
    for n, (dx, dy, kk) in enumerate(plane):
        if kk is k:
            same = same + sqx[n]
        else:
            cross = cross + sqx[n]
    lane = lax.broadcasted_iota(jnp.int32, (16, 128), 1) // 32
    for m in range(2):
        master_ref, copy_ref, step_ref, moment_ref, rows_ref, cols_ref = made[m::2]
        weight_old, moment_old, rows_old, cols_old = held[9 + m :: 2]
        square = jnp.where(k == m, same, cross)
        scale = jnp.sqrt(D * HW / (square + 1.0))
        twice = scale * scale
        by_row = (1.0 - stat_decay) / HW * twice
        by_col = (1.0 - stat_decay) / D * twice
        for i in range(4):
            sums = []
            for n in range(4):
                total = orv[m, n, 0, i].astype(f32)
                for q in range(1, 4):
                    total = total + orv[m, n, q, i].astype(f32)
                sums.append(by_row * total)
            for e in range(4):
                block = sums[0] if e == 0 else pltpu.roll(sums[0], (128 - 32 * e) % 128, 1)
                for n in range(1, 4):
                    turn = (32 * (n - e)) % 128
                    block = jnp.where(lane == n, pltpu.roll(sums[n], turn, 1) if turn else sums[n], block)
                lanes = pl.ds(pl.multiple_of(zat(chunks[i][e]) * 128, 128), 128)
                rows_ref[:, lanes] = stat_decay * rows_old[:, lanes] + block
        for h in range(2):
            lanes = slice(h * 128, (h + 1) * 128)
            precond = scale * pre[m, h]
            moment = moment_decay * moment_old[:, lanes] + (1.0 - moment_decay) * precond
            step = moment_decay * moment + (1.0 - moment_decay) * precond
            master = weight_old[:, lanes] - learn_rate * step
            moment_ref[:, lanes] = moment
            step_ref[:, lanes] = step
            master_ref[:, lanes] = master
            copy_ref[:, lanes] = master.astype(bf16)
            for n in range(2):
                part = slice(64 * n, 64 * n + 64)
                cols_ref[h, part] = stat_decay * cols_old[h, part] + by_col * colin[m, h, n].astype(f32)
    net.drain()


def store(*refs):
    sems = refs[24]
    moves = [pltpu.make_async_copy(u, v, sems.at[n]) for n, (u, v) in enumerate(zip(refs[:12], refs[12:24]))]
    for c in moves:
        c.start()
    for c in moves:
        c.wait()


def on_device(inputs, qg, fg, fp, lb, qw, fw, qm, fm, qr, fr, qc, fc, qrr, frr, qcr, fcr):
    hbm = pl.BlockSpec(memory_space=pltpu.HBM)
    vm = pl.BlockSpec(memory_space=pltpu.VMEM)
    s = lambda shape, kind=bf16: pltpu.VMEM(shape, kind)
    given = (inputs, qg, fg, fp, lb.reshape(1, -1), qrr, frr, qcr, fcr, qw, fw, qm, fm, qr, fr, qc, fc)
    like = (qw, fw, qg, fg, qw, fw, qw, fw, qr, fr, qc, fc)
    shapes = [(v.shape if v.ndim != 2 or v.shape[1] == D else (16, 256), v.dtype) for v in like]
    made = pl.pallas_call(
        kernel,
        out_shape=tuple(pltpu.VMEM(*v) for v in shapes),
        in_specs=[hbm] * 17,
        out_specs=(vm,) * 12,
        scratch_shapes=[s(v.shape, v.dtype) for v in given]
        + [
            s((4, 128, 128)),
            s((4, 4, 128, 128)),
            s((4, 2, 128, 256)),
            s((2, 4, 4, 16, 128)),
            s((4, 2, 4, 16, 128)),
            s((4, 4, 32, 256), f32),
            s((4, 128, 256), f32),
            s((4, 128, 256), f32),
            s((4, 4, 32, 256)),
            s((7, 32, 256)),
            s((10, 32, 256)),
            s((3, 32, 256)),
            s((6, 32, 256)),
            s((4, 32, 256)),
            s((16, 32, 256)),
            s((4, 2, 4, 16, 128)),
            s((2, 4, 4, 4, 16, 128)),
            s((4, 2, 16, 256)),
            s((2, 4, 16, 256)),
            s((2, 2, 64, HEAD)),
            s((4, 2, 64, HEAD)),
            s((2, 64, HEAD)),
            s((2, 2, 2, 64, HEAD)),
            s((1, 1, 128), f32),
            s((31, 1, 128), f32),
            pltpu.SemaphoreType.DMA((2,)),
            s((TILES, 16, 128)),
            pltpu.SemaphoreType.DMA,
            pltpu.SemaphoreType.DMA((SEMS,)),
            pltpu.SemaphoreType.DMA((len(given),)),
        ],
        compiler_params=pltpu.CompilerParams(collective_id=0, has_side_effects=True),
        name="exchange",
    )(*given)
    return pl.pallas_call(
        store,
        out_shape=tuple(jax.ShapeDtypeStruct(*v) for v in shapes),
        in_specs=[vm] * 12,
        out_specs=(hbm,) * 12,
        scratch_shapes=[pltpu.SemaphoreType.DMA((12,))],
        name="store",
    )(*(pltpu.with_memory_space_constraint(v, pltpu.VMEM) for v in made))


def solution(mesh):
    split = Mesh(mesh.devices.reshape(16, 4, 2, mesh.shape["tp"]), ("fs_0", "fs_1", "fs_2", "tp"))
    both, rows, cols = P(FS, "tp"), P(FS, None), P("tp", None, None)
    return jax.shard_map(
        on_device,
        mesh=split,
        in_specs=(both,) * 4 + (P("tp"),) + (both,) * 4 + (rows,) * 2 + (cols,) * 2 + (rows,) * 2 + (cols,) * 2,
        out_specs=(both,) * 8 + (rows,) * 2 + (cols,) * 2,
        check_vma=False,
    )
```

```python
import jax
import jax.numpy as jnp
from jax import lax
from jax.experimental import pallas as pl
from jax.experimental.pallas import tpu as pltpu
from jax.sharding import Mesh
from jax.sharding import PartitionSpec as P

D = 2048
HW = 1024
HEAD = 128
FS = ("fs_0", "fs_1", "fs_2")
MESH = pl.DeviceIdType.MESH
SEMS = 27
TILES = 698

stat_decay = 0.9
moment_decay = 0.9
learn_rate = 0.02
highest = lax.Precision.HIGHEST
f32 = jnp.float32
bf16 = jnp.bfloat16


class Net:
    def __init__(self, send, recv, room, other):
        self.send, self.recv, self.room, self.other = send, recv, room, other
        self.names, self.sent, self.waited = {}, {}, {}

    def sem(self, name):
        return self.recv.at[self.names.setdefault(name, len(self.names))]

    def copy(self, name, src, dst, count=True, **where):
        pltpu.make_async_remote_copy(
            src_ref=src,
            dst_ref=dst,
            send_sem=self.send,
            recv_sem=self.sem(name),
            device_id=where,
            device_id_type=MESH,
        ).start()
        size = src.dtype.itemsize
        for n in src.shape:
            size *= n
        assert size % 4096 == 0
        if count:
            self.sent[name] = self.sent.get(name, 0) + size // 4096

    def tiles(self, sem, tiles):
        room = self.room.at[pl.ds(0, tiles)]
        return pltpu.make_async_remote_copy(
            src_ref=room,
            dst_ref=room,
            send_sem=self.send,
            recv_sem=sem,
            device_id=self.other,
            device_id_type=MESH,
        )

    def wait(self, name):
        assert name not in self.waited
        self.waited[name] = self.sent[name]
        self.tiles(self.sem(name), self.sent[name]).wait_recv()

    def drain(self):
        assert self.waited == self.sent
        total = sum(self.sent.values())
        assert (len(self.names), total) == (SEMS, TILES), (len(self.names), total)
        self.tiles(self.recv.at[0], total).wait_send()


def dot(a, b):
    return jnp.dot(a, b, preferred_element_type=f32)


def kernel(
    *refs,
):
    given, refs = refs[:17], refs[17:]
    made, refs = refs[:12], refs[12:]
    held, refs = refs[:17], refs[17:]
    x_ref, qg_ref, fg_ref, fp_ref, lb_ref, rq_ref, rf_ref, cq_ref, cf_ref = held[:9]
    (
    xt, xx, gx, rpack, rin, pmine, pout, pin, gp, rd, ru, sb, rf, gz, gc, o, orv, lp, lin, gram, gin, quarter, colin, sq, sqx, sqroom, sums, sqsem,
    room, send, recv, loads,
    ) = refs
    z, x, k, y = (lax.axis_index(n) for n in ("fs_0", "fs_1", "fs_2", "tp"))
    ko, b = 1 - k, lax.rem(z, 2)
    at = lambda v, n, m: lax.rem(v + n + m, m)
    ym, yp, y2 = at(y, -1, 4), at(y, 1, 4), at(y, 2, 4)
    zat = lambda n: at(z, n, 16)
    net = Net(send, recv, room, dict(fs_2=ko))
    steps = (2, 1, 3)
    plane = [
        (dx, dy, kk)
        for dx, dy in ((2, 2), (1, 2), (3, 2), (2, 1), (2, 3), (1, 1), (3, 3), (1, 3), (3, 1), (2, 0), (0, 2), (1, 0), (0, 1), (3, 0), (0, 3), (0, 0))
        for kk in (k, ko)
        if (dx, dy) != (0, 0) or kk is ko
    ]

    barrier = pltpu.get_barrier_semaphore()
    partners = [dict(fs_0=zat(n)) for n in (3, -3, 2, -2, 1, -1)]
    partners += [dict(fs_1=at(x, d, 4)) for d in steps]
    partners += [dict(tp=at(y, d, 4)) for d in steps]
    partners += [dict(fs_2=ko)]
    for who in partners:
        pl.semaphore_signal(barrier, inc=1, device_id=who, device_id_type=MESH)

    load = [pltpu.make_async_copy(u, v, loads.at[n]) for n, (u, v) in enumerate(zip(given, held))]
    for c in load:
        c.start()
    load[0].wait()
    for n in range(4):
        turned = x_ref[:, n * 128 : (n + 1) * 128].T
        for q in range(4):
            xt[q, n * 32 : (n + 1) * 32] = turned[q * 32 : (q + 1) * 32]
    xx[y, x] = xt[x]
    for c in load[1:5]:
        c.wait()
    gx[x, 0] = qg_ref[...]
    gate = jax.nn.sigmoid(fp_ref[...].astype(f32))
    gx[x, 1] = (fg_ref[...].astype(f32) * (1.0 - lb_ref[...]) * gate * (1.0 - gate)).astype(bf16)
    pl.semaphore_wait(barrier, len(partners))

    for d in steps:
        net.copy(("x", d), xt.at[at(x, d, 4)], xx.at[y, x], fs_1=at(x, d, 4))

    def ysend(n):
        for d in steps:
            net.copy(("y", d), xx.at[y, n], xx.at[y, n], tp=at(y, d, 4))

    ysend(x)
    halves = (pl.ds(0, 64), pl.ds(64, 64))

    def gcopy(name, n, m, h, d):
        net.copy(name, gx.at[n, m, h], gx.at[n, m, h], fs_1=at(x, d, 4))

    for i, h in enumerate(halves):
        gcopy(("gq", i), x, 0, h, 1)
        gcopy(("gf", i), x, 1, h, -1)
    for h in halves:
        gcopy("g", x, 1, h, 1)
        gcopy("g", x, 0, h, -1)
    for c in load[5:9]:
        c.wait()
    for m, ref in enumerate((rq_ref, rf_ref)):
        for n in range(4):
            wide = ref[:, n * 512 : (n + 1) * 512].astype(f32)
            for q in range(4):
                strips = [wide[:, w * 128 + q * 32 : w * 128 + (q + 1) * 32] for w in range(4)]
                rpack[m, q, n] = jnp.concatenate(strips, axis=1).astype(bf16)
    rin[x, k] = rpack[k, x]
    net.copy("r", rpack.at[ko, x], rin.at[x, k], fs_2=ko)
    for d in (1, 3, 2):
        net.wait(("x", d))
        ysend(at(x, -d, 4))

    def product(j, a):
        lhs = jnp.concatenate([xx[a, n] for n in range(4)], axis=1)
        pout[a] = dot(lhs, gx[:, ko].reshape(512, 256))
        pmine[a] = dot(lhs, gx[:, k].reshape(512, 256)).reshape(4, 32, 256)
        net.copy(("p", j), pout.at[a], pin.at[a], fs_2=ko)

    def scatter(j, a):
        net.wait(("p", j))
        total = pmine[a] + pin[a].reshape(4, 32, 256)
        pmine[a] = total
        gp[a] = total.astype(bf16)
        for q in range(4):
            t = 4 * a + q
            d = at(t, -z, 16)
            up = (d == 4) | (d == 5) | (d == 7) | (d == 8)
            down = (d == 9) | (d == 11) | (d == 12)
            direct = (d == 1) | (d == 2) | (d == 3) | (d == 13) | (d == 14) | (d == 15)

            @pl.when(up | down)
            def _():
                slot = d - jnp.where(up, 4, 3)
                relay = lax.rem(t + jnp.where(up, 10, 6), 16)
                net.copy("u", gp.at[a, q], ru.at[slot], count=False, fs_0=relay)

            @pl.when(direct)
            def _():
                net.copy("s", gp.at[a, q], rd.at[lax.rem(d + 3, 16)], count=False, fs_0=t)

    for i, h in enumerate(halves):
        net.wait(("gq", i))
        gcopy("g", at(x, -1, 4), 0, h, 1)
        net.wait(("gf", i))
        gcopy("g", at(x, 1, 4), 1, h, -1)
    net.wait("g")
    product(0, y)
    net.wait(("y", 1))
    product(1, ym)
    net.wait(("y", 3))
    product(2, yp)
    scatter(0, y)
    net.wait(("y", 2))
    product(3, y2)
    scatter(1, ym)
    scatter(2, yp)
    scatter(3, y2)
    for dx in steps:
        for m, kk in ((k, k), (ko, ko)):
            net.copy("r", rpack.at[m, at(x, dx, 4)], rin.at[x, k], fs_1=at(x, dx, 4), fs_2=kk)
    net.sent["s"], net.sent["u"] = 6 * 4, 7 * 4
    net.wait("u")
    part = lambda t: pmine[t // 4, lax.rem(t, 4)]
    net.wait("s")
    for n, e, slots in ((0, 6, (0, 1, 3, 4)), (1, -6, (6, 8, 9))):
        total = part(zat(e))
        for i in slots:
            total = total + ru[i].astype(f32)
        sb[n] = total.astype(bf16)
        net.copy("f", sb.at[n], rf.at[2 + 2 * n], fs_0=zat(e))
        net.copy("f", sb.at[n], rf.at[3 + 2 * n], fs_0=zat(2 * e))
    total = part(z)
    for i in (0, 1, 2, 4, 5, 6):
        total = total + rd[i].astype(f32)
    sb[2] = total.astype(bf16)
    net.copy("f", sb.at[2], rf.at[0], fs_0=zat(6))
    net.copy("f", sb.at[2], rf.at[1], fs_0=zat(-6))
    net.wait("f")

    def joined(mid, above, below):
        return (mid.astype(f32) + above.astype(f32) + below.astype(f32)).astype(bf16)

    mine = joined(sb[2], rf[4], rf[2])
    gc[z] = mine
    gz[x] = mine
    gc[zat(6)] = joined(rf[1], rf[5], sb[0])
    gc[zat(-6)] = joined(rf[0], sb[1], rf[3])

    chunks = ((0, 6, -6, 1), (7, -5, -1, 5), (-7, 2, -8, -4), (-2, 4, 3, -3))
    for d in steps:
        net.copy("gz", gz.at[x], gz.at[x], fs_1=at(x, d, 4))
    for name, n, held_here in (
        ("first", 1, (0, 6, -6)), ("first", -1, (0, 6, -6)), ("last", 3, (0,)), ("last", -3, (0,)),
        ("last", 2, (0, 6, -6)), ("last", -2, (0, -6)),
    ):
        for e in held_here:
            net.copy(("z", name), gc.at[zat(e)], gc.at[zat(e)], fs_0=zat(n))
    net.wait("r")
    net.wait(("z", "first"))
    net.wait("gz")
    rows = gz[...].reshape(128, 256)

    def outer(i):
        cols = jnp.concatenate([gc[zat(e)] for e in chunks[i]], axis=0)
        block = lax.dot_general(rows, cols, (((1,), (1,)), ((), ())), preferred_element_type=f32).astype(bf16)
        for q in range(8):
            o[q // 2, q % 2, i] = block[q * 16 : (q + 1) * 16]

    def osend(group, h):
        orv[k, x, y, h] = o[x, k, h]
        for dx, dy, kk in plane:
            to_x, to_y = at(x, dx, 4), at(y, dy, 4)
            net.copy(("o", group), o.at[to_x, kk, h], orv.at[k, x, y, h], fs_1=to_x, tp=to_y, fs_2=kk)

    outer(0)
    outer(1)
    osend(0, pl.ds(0, 2))
    net.wait(("z", "last"))
    whole = gc[...].reshape(512, 256)
    for h in range(2):
        lanes = slice(h * 128, (h + 1) * 128)
        turned = whole[:, lanes]
        both = lax.dot_general(turned, turned, (((0,), (0,)), ((), ())), preferred_element_type=f32).astype(bf16)
        gram[h, 0] = both[:64]
        gram[h, 1] = both[64:]
    for d in steps:
        net.copy("gram", gram.at[b], gin.at[x], fs_1=at(x, d, 4))
    wide = whole.astype(f32)
    square = jnp.sum((wide * wide).reshape(64, 8, 256), axis=0)
    square = jnp.sum(square, axis=(0, 1), keepdims=True)
    sq[0] = jnp.broadcast_to(square, (1, 128))
    outer(2)
    outer(3)
    sqx[k, 4 * x + y] = sq[0]
    for dx, dy, kk in plane:
        pltpu.make_async_remote_copy(
            src_ref=sq.at[0],
            dst_ref=sqx.at[k, 4 * x + y],
            send_sem=sqsem.at[0],
            recv_sem=sqsem.at[1],
            device_id=dict(fs_1=at(x, dx, 4), tp=at(y, dy, 4), fs_2=kk),
            device_id_type=MESH,
        ).start()
    osend(1, pl.ds(2, 2))
    roots = rin[...].reshape(8, 4, 16, 128)
    roots = jnp.concatenate(
        [jnp.concatenate([roots[q, n] for n in range(4)], axis=1) for q in range(8)], axis=0
    )
    left = dot(roots, whole)
    lp[...] = left.reshape(4, 2, 16, 256).astype(bf16)
    lin[k, x] = lp[x, k]
    for dx in (2, 1, 3, 0):
        for kk in (k, ko):
            if dx or kk is ko:
                to_x = at(x, dx, 4)
                net.copy("l", lp.at[to_x, kk], lin.at[k, x], fs_1=to_x, fs_2=kk)
    net.wait("gram")
    gin[x] = gram[b]
    total = gin[0].astype(f32) + gin[1].astype(f32) + gin[2].astype(f32) + gin[3].astype(f32)
    quarter[...] = total.astype(bf16)
    for n, e in ((0, 1), (1, -1)):
        for kk in (k, ko):
            net.copy("col", quarter.at[n], colin.at[k, b, n], fs_0=zat(e), fs_2=kk)
    net.copy("col", quarter, colin.at[k, b], fs_2=ko)
    colin[k, b] = quarter[...]
    net.wait("l")
    pre = {}
    for m, ref in enumerate((cq_ref, cf_ref)):
        value = lin[m, 0].astype(f32)
        for n in range(1, 4):
            value = value + lin[m, n].astype(f32)
        high = value.astype(bf16)
        low = (value - high.astype(f32)).astype(bf16)
        for h in range(2):
            lanes = slice(h * 128, (h + 1) * 128)
            pre[m, h] = dot(high[:, lanes], ref[h]) + dot(low[:, lanes], ref[h])
    for c in load[9:]:
        c.wait()
    lane = lax.broadcasted_iota(jnp.int32, (16, 128), 1) // 32

    def gather_rows(group):
        net.wait(("o", group))
        for m in range(2):
            for i in (2 * group, 2 * group + 1):
                parts = []
                for n in range(4):
                    total = orv[m, n, 0, i].astype(f32)
                    for q in range(1, 4):
                        total = total + orv[m, n, q, i].astype(f32)
                    parts.append(total)
                for e in range(4):
                    block = parts[0] if e == 0 else pltpu.roll(parts[0], (128 - 32 * e) % 128, 1)
                    for n in range(1, 4):
                        turn = (32 * (n - e)) % 128
                        block = jnp.where(lane == n, pltpu.roll(parts[n], turn, 1) if turn else parts[n], block)
                    sums[m, i, e] = block

    gather_rows(0)
    gather_rows(1)
    net.wait("col")
    squares = pltpu.make_async_remote_copy(
        src_ref=sqroom,
        dst_ref=sqroom,
        send_sem=sqsem.at[0],
        recv_sem=sqsem.at[1],
        device_id=dict(fs_2=ko),
        device_id_type=MESH,
    )
    squares.wait_recv()
    squares.wait_send()
    for m in range(2):
        master_ref, copy_ref, step_ref, moment_ref, rows_ref, cols_ref = made[m::2]
        weight_old, moment_old, rows_old, cols_old = held[9 + m :: 2]
        square = sqx[m, 0]
        for n in range(1, 16):
            square = square + sqx[m, n]
        scale = jnp.sqrt(D * HW / (square + 1.0))
        twice = scale * scale
        by_row = (1.0 - stat_decay) / HW * twice
        by_col = (1.0 - stat_decay) / D * twice
        for i in range(4):
            for e in range(4):
                lanes = pl.ds(pl.multiple_of(zat(chunks[i][e]) * 128, 128), 128)
                rows_ref[:, lanes] = stat_decay * rows_old[:, lanes] + by_row * sums[m, i, e]
        for h in range(2):
            lanes = slice(h * 128, (h + 1) * 128)
            precond = scale * pre[m, h]
            moment = moment_decay * moment_old[:, lanes] + (1.0 - moment_decay) * precond
            step = moment_decay * moment + (1.0 - moment_decay) * precond
            master = weight_old[:, lanes] - learn_rate * step
            moment_ref[:, lanes] = moment
            step_ref[:, lanes] = step
            master_ref[:, lanes] = master
            copy_ref[:, lanes] = master.astype(bf16)
            for n in range(2):
                part = slice(64 * n, 64 * n + 64)
                cols_ref[h, part] = stat_decay * cols_old[h, part] + by_col * colin[m, h, n].astype(f32)
    net.drain()


def store(*refs):
    sems = refs[24]
    moves = [pltpu.make_async_copy(u, v, sems.at[n]) for n, (u, v) in enumerate(zip(refs[:12], refs[12:24]))]
    for c in moves:
        c.start()
    for c in moves:
        c.wait()


def on_device(inputs, qg, fg, fp, lb, qw, fw, qm, fm, qr, fr, qc, fc, qrr, frr, qcr, fcr):
    hbm = pl.BlockSpec(memory_space=pltpu.HBM)
    vm = pl.BlockSpec(memory_space=pltpu.VMEM)
    s = lambda shape, kind=bf16: pltpu.VMEM(shape, kind)
    given = (inputs, qg, fg, fp, lb.reshape(1, -1), qrr, frr, qcr, fcr, qw, fw, qm, fm, qr, fr, qc, fc)
    like = (qw, fw, qg, fg, qw, fw, qw, fw, qr, fr, qc, fc)
    shapes = [(v.shape if v.ndim != 2 or v.shape[1] == D else (16, 256), v.dtype) for v in like]
    made = pl.pallas_call(
        kernel,
        out_shape=tuple(pltpu.VMEM(*v) for v in shapes),
        in_specs=[hbm] * 17,
        out_specs=(vm,) * 12,
        scratch_shapes=[s(v.shape, v.dtype) for v in given]
        + [
            s((4, 128, 128)),
            s((4, 4, 128, 128)),
            s((4, 2, 128, 256)),
            s((2, 4, 4, 16, 128)),
            s((4, 2, 4, 16, 128)),
            s((4, 4, 32, 256), f32),
            s((4, 128, 256), f32),
            s((4, 128, 256), f32),
            s((4, 4, 32, 256)),
            s((7, 32, 256)),
            s((10, 32, 256)),
            s((3, 32, 256)),
            s((6, 32, 256)),
            s((4, 32, 256)),
            s((16, 32, 256)),
            s((4, 2, 4, 16, 128)),
            s((2, 4, 4, 4, 16, 128)),
            s((4, 2, 16, 256)),
            s((2, 4, 16, 256)),
            s((2, 2, 64, HEAD)),
            s((4, 2, 64, HEAD)),
            s((2, 64, HEAD)),
            s((2, 2, 2, 64, HEAD)),
            s((1, 1, 128), f32),
            s((2, 16, 1, 128), f32),
            s((31, 1, 128), f32),
            s((2, 4, 4, 16, 128), f32),
            pltpu.SemaphoreType.DMA((2,)),
            s((TILES, 16, 128)),
            pltpu.SemaphoreType.DMA,
            pltpu.SemaphoreType.DMA((SEMS,)),
            pltpu.SemaphoreType.DMA((len(given),)),
        ],
        compiler_params=pltpu.CompilerParams(collective_id=0, has_side_effects=True),
        name="exchange",
    )(*given)
    return pl.pallas_call(
        store,
        out_shape=tuple(jax.ShapeDtypeStruct(*v) for v in shapes),
        in_specs=[vm] * 12,
        out_specs=(hbm,) * 12,
        scratch_shapes=[pltpu.SemaphoreType.DMA((12,))],
        name="store",
    )(*(pltpu.with_memory_space_constraint(v, pltpu.VMEM) for v in made))


def solution(mesh):
    split = Mesh(mesh.devices.reshape(16, 4, 2, mesh.shape["tp"]), ("fs_0", "fs_1", "fs_2", "tp"))
    both, rows, cols = P(FS, "tp"), P(FS, None), P("tp", None, None)
    return jax.shard_map(
        on_device,
        mesh=split,
        in_specs=(both,) * 4 + (P("tp"),) + (both,) * 4 + (rows,) * 2 + (cols,) * 2 + (rows,) * 2 + (cols,) * 2,
        out_specs=(both,) * 8 + (rows,) * 2 + (cols,) * 2,
        check_vma=False,
    )
```

```python
import jax
import jax.numpy as jnp
from jax import lax
from jax.experimental import pallas as pl
from jax.experimental.pallas import tpu as pltpu
from jax.sharding import Mesh
from jax.sharding import PartitionSpec as P

D = 2048
HW = 1024
HEAD = 128
FS = ("fs_0", "fs_1", "fs_2")
MESH = pl.DeviceIdType.MESH
SEMS = 27
TILES = 698

stat_decay = 0.9
moment_decay = 0.9
learn_rate = 0.02
highest = lax.Precision.HIGHEST
f32 = jnp.float32
bf16 = jnp.bfloat16


class Net:
    def __init__(self, send, recv, room, other):
        self.send, self.recv, self.room, self.other = send, recv, room, other
        self.names, self.sent, self.waited = {}, {}, {}

    def sem(self, name):
        return self.recv.at[self.names.setdefault(name, len(self.names))]

    def copy(self, name, src, dst, count=True, **where):
        pltpu.make_async_remote_copy(
            src_ref=src,
            dst_ref=dst,
            send_sem=self.send,
            recv_sem=self.sem(name),
            device_id=where,
            device_id_type=MESH,
        ).start()
        size = src.dtype.itemsize
        for n in src.shape:
            size *= n
        assert size % 4096 == 0
        if count:
            self.sent[name] = self.sent.get(name, 0) + size // 4096

    def tiles(self, sem, tiles):
        room = self.room.at[pl.ds(0, tiles)]
        return pltpu.make_async_remote_copy(
            src_ref=room,
            dst_ref=room,
            send_sem=self.send,
            recv_sem=sem,
            device_id=self.other,
            device_id_type=MESH,
        )

    def wait(self, name):
        assert name not in self.waited
        self.waited[name] = self.sent[name]
        self.tiles(self.sem(name), self.sent[name]).wait_recv()

    def drain(self):
        assert self.waited == self.sent
        total = sum(self.sent.values())
        assert (len(self.names), total) == (SEMS, TILES), (len(self.names), total)
        self.tiles(self.recv.at[0], total).wait_send()


def dot(a, b):
    return jnp.dot(a, b, preferred_element_type=f32)


def kernel(
    *refs,
):
    given, refs = refs[:17], refs[17:]
    made, refs = refs[:12], refs[12:]
    held, refs = refs[:17], refs[17:]
    x_ref, qg_ref, fg_ref, fp_ref, lb_ref, rq_ref, rf_ref, cq_ref, cf_ref = held[:9]
    (
    xt, xx, gx, rpack, rin, pmine, pout, pin, gp, rd, ru, sb, rf, gz, gc, o, orv, lp, lin, gram, gin, quarter, colin, sq, sqx, sqroom, sums, sqsem, tokens,
    room, send, recv, loads,
    ) = refs
    z, x, k, y = (lax.axis_index(n) for n in ("fs_0", "fs_1", "fs_2", "tp"))
    ko, b = 1 - k, lax.rem(z, 2)
    at = lambda v, n, m: lax.rem(v + n + m, m)
    ym, yp, y2 = at(y, -1, 4), at(y, 1, 4), at(y, 2, 4)
    zat = lambda n: at(z, n, 16)
    net = Net(send, recv, room, dict(fs_2=ko))
    steps = (2, 1, 3)
    plane = [
        (dx, dy, kk)
        for dx, dy in ((2, 2), (1, 2), (3, 2), (2, 1), (2, 3), (1, 1), (3, 3), (1, 3), (3, 1), (2, 0), (0, 2), (1, 0), (0, 1), (3, 0), (0, 3), (0, 0))
        for kk in (k, ko)
        if (dx, dy) != (0, 0) or kk is ko
    ]

    barrier = pltpu.get_barrier_semaphore()
    partners = [dict(fs_1=at(x, d, 4)) for d in steps]
    partners += [dict(tp=at(y, d, 4)) for d in steps]
    partners += [dict(fs_0=zat(n)) for n in (1, -1)] + [dict(fs_2=ko)]
    for who in partners:
        pl.semaphore_signal(barrier, inc=1, device_id=who, device_id_type=MESH)

    load = [pltpu.make_async_copy(u, v, loads.at[n]) for n, (u, v) in enumerate(zip(given, held))]
    for c in load:
        c.start()
    load[0].wait()
    for n in range(4):
        turned = x_ref[:, n * 128 : (n + 1) * 128].T
        for q in range(4):
            xt[q, n * 32 : (n + 1) * 32] = turned[q * 32 : (q + 1) * 32]
    xx[y, x] = xt[x]
    for c in load[1:5]:
        c.wait()
    gx[x, 0] = qg_ref[...]
    gate = jax.nn.sigmoid(fp_ref[...].astype(f32))
    gx[x, 1] = (fg_ref[...].astype(f32) * (1.0 - lb_ref[...]) * gate * (1.0 - gate)).astype(bf16)
    pl.semaphore_wait(barrier, len(partners))

    for d in steps:
        net.copy(("x", d), xt.at[at(x, d, 4)], xx.at[y, x], fs_1=at(x, d, 4))

    def ysend(n):
        for d in steps:
            net.copy(("y", d), xx.at[y, n], xx.at[y, n], tp=at(y, d, 4))

    ysend(x)

    def token(n):
        for e in (1, -1):
            pl.semaphore_signal(tokens.at[n], inc=1, device_id=dict(fs_0=zat(e)), device_id_type=MESH)

    token(0)
    halves = (pl.ds(0, 64), pl.ds(64, 64))

    def gcopy(name, n, m, h, d):
        net.copy(name, gx.at[n, m, h], gx.at[n, m, h], fs_1=at(x, d, 4))

    for i, h in enumerate(halves):
        gcopy(("gq", i), x, 0, h, 1)
        gcopy(("gf", i), x, 1, h, -1)
    for h in halves:
        gcopy("g", x, 1, h, 1)
        gcopy("g", x, 0, h, -1)
    for c in load[5:9]:
        c.wait()
    for m, ref in enumerate((rq_ref, rf_ref)):
        for n in range(4):
            wide = ref[:, n * 512 : (n + 1) * 512].astype(f32)
            for q in range(4):
                strips = [wide[:, w * 128 + q * 32 : w * 128 + (q + 1) * 32] for w in range(4)]
                rpack[m, q, n] = jnp.concatenate(strips, axis=1).astype(bf16)
    rin[x, k] = rpack[k, x]
    net.copy("r", rpack.at[ko, x], rin.at[x, k], fs_2=ko)
    for d in (1, 3, 2):
        net.wait(("x", d))
        ysend(at(x, -d, 4))

    def product(j, a):
        lhs = jnp.concatenate([xx[a, n] for n in range(4)], axis=1)
        pout[a] = dot(lhs, gx[:, ko].reshape(512, 256))
        pmine[a] = dot(lhs, gx[:, k].reshape(512, 256)).reshape(4, 32, 256)
        net.copy(("p", j), pout.at[a], pin.at[a], fs_2=ko)

    def scatter(j, a):
        net.wait(("p", j))
        total = pmine[a] + pin[a].reshape(4, 32, 256)
        pmine[a] = total
        gp[a] = total.astype(bf16)
        for q in range(4):
            t = 4 * a + q
            d = at(t, -z, 16)
            up = (d == 4) | (d == 5) | (d == 7) | (d == 8)
            down = (d == 9) | (d == 11) | (d == 12)
            direct = (d == 1) | (d == 2) | (d == 3) | (d == 13) | (d == 14) | (d == 15)

            @pl.when(up | down)
            def _():
                slot = d - jnp.where(up, 4, 3)
                relay = lax.rem(t + jnp.where(up, 10, 6), 16)
                net.copy("u", gp.at[a, q], ru.at[slot], count=False, fs_0=relay)

            @pl.when(direct)
            def _():
                net.copy("s", gp.at[a, q], rd.at[lax.rem(d + 3, 16)], count=False, fs_0=t)

    pl.semaphore_wait(tokens.at[0], 2)
    token(1)
    for i, h in enumerate(halves):
        net.wait(("gq", i))
        gcopy("g", at(x, -1, 4), 0, h, 1)
        net.wait(("gf", i))
        gcopy("g", at(x, 1, 4), 1, h, -1)
    pl.semaphore_wait(tokens.at[1], 2)
    net.wait("g")
    product(0, y)
    net.wait(("y", 1))
    product(1, ym)
    net.wait(("y", 3))
    product(2, yp)
    net.wait(("y", 2))
    product(3, y2)
    scatter(0, y)
    scatter(1, ym)
    scatter(2, yp)
    scatter(3, y2)
    for dx in steps:
        for m, kk in ((k, k), (ko, ko)):
            net.copy("r", rpack.at[m, at(x, dx, 4)], rin.at[x, k], fs_1=at(x, dx, 4), fs_2=kk)
    net.sent["s"], net.sent["u"] = 6 * 4, 7 * 4
    net.wait("u")
    part = lambda t: pmine[t // 4, lax.rem(t, 4)]
    net.wait("s")
    for n, e, slots in ((0, 6, (0, 1, 3, 4)), (1, -6, (6, 8, 9))):
        total = part(zat(e))
        for i in slots:
            total = total + ru[i].astype(f32)
        sb[n] = total.astype(bf16)
        net.copy("f", sb.at[n], rf.at[2 + 2 * n], fs_0=zat(e))
        net.copy("f", sb.at[n], rf.at[3 + 2 * n], fs_0=zat(2 * e))
    total = part(z)
    for i in (0, 1, 2, 4, 5, 6):
        total = total + rd[i].astype(f32)
    sb[2] = total.astype(bf16)
    net.copy("f", sb.at[2], rf.at[0], fs_0=zat(6))
    net.copy("f", sb.at[2], rf.at[1], fs_0=zat(-6))
    net.wait("f")

    def joined(mid, above, below):
        return (mid.astype(f32) + above.astype(f32) + below.astype(f32)).astype(bf16)

    mine = joined(sb[2], rf[4], rf[2])
    gc[z] = mine
    gz[x] = mine
    gc[zat(6)] = joined(rf[1], rf[5], sb[0])
    gc[zat(-6)] = joined(rf[0], sb[1], rf[3])

    chunks = ((0, 6, -6, 1), (7, -5, -1, 5), (-7, 2, -8, -4), (-2, 4, 3, -3))
    for d in steps:
        net.copy("gz", gz.at[x], gz.at[x], fs_1=at(x, d, 4))
    for name, n, held_here in (
        ("first", 1, (0, 6, -6)), ("first", -1, (0, 6, -6)), ("last", 3, (0,)), ("last", -3, (0,)),
        ("last", 2, (0, 6, -6)), ("last", -2, (0, -6)),
    ):
        for e in held_here:
            net.copy(("z", name), gc.at[zat(e)], gc.at[zat(e)], fs_0=zat(n))
    net.wait("r")
    net.wait(("z", "first"))
    net.wait("gz")
    rows = gz[...].reshape(128, 256)

    def outer(i):
        cols = jnp.concatenate([gc[zat(e)] for e in chunks[i]], axis=0)
        block = lax.dot_general(rows, cols, (((1,), (1,)), ((), ())), preferred_element_type=f32).astype(bf16)
        for q in range(8):
            o[q // 2, q % 2, i] = block[q * 16 : (q + 1) * 16]

    def osend(group, h):
        orv[k, x, y, h] = o[x, k, h]
        for dx, dy, kk in plane:
            to_x, to_y = at(x, dx, 4), at(y, dy, 4)
            net.copy(("o", group), o.at[to_x, kk, h], orv.at[k, x, y, h], fs_1=to_x, tp=to_y, fs_2=kk)

    outer(0)
    outer(1)
    osend(0, pl.ds(0, 2))
    net.wait(("z", "last"))
    whole = gc[...].reshape(512, 256)
    for h in range(2):
        lanes = slice(h * 128, (h + 1) * 128)
        turned = whole[:, lanes]
        both = lax.dot_general(turned, turned, (((0,), (0,)), ((), ())), preferred_element_type=f32).astype(bf16)
        gram[h, 0] = both[:64]
        gram[h, 1] = both[64:]
    for d in steps:
        net.copy("gram", gram.at[b], gin.at[x], fs_1=at(x, d, 4))
    wide = whole.astype(f32)
    square = jnp.sum((wide * wide).reshape(64, 8, 256), axis=0)
    square = jnp.sum(square, axis=(0, 1), keepdims=True)
    sq[0] = jnp.broadcast_to(square, (1, 128))
    outer(2)
    outer(3)
    sqx[k, 4 * x + y] = sq[0]
    for dx, dy, kk in plane:
        pltpu.make_async_remote_copy(
            src_ref=sq.at[0],
            dst_ref=sqx.at[k, 4 * x + y],
            send_sem=sqsem.at[0],
            recv_sem=sqsem.at[1],
            device_id=dict(fs_1=at(x, dx, 4), tp=at(y, dy, 4), fs_2=kk),
            device_id_type=MESH,
        ).start()
    osend(1, pl.ds(2, 2))
    roots = rin[...].reshape(8, 4, 16, 128)
    roots = jnp.concatenate(
        [jnp.concatenate([roots[q, n] for n in range(4)], axis=1) for q in range(8)], axis=0
    )
    left = dot(roots, whole)
    lp[...] = left.reshape(4, 2, 16, 256).astype(bf16)
    lin[k, x] = lp[x, k]
    for dx in (2, 1, 3, 0):
        for kk in (k, ko):
            if dx or kk is ko:
                to_x = at(x, dx, 4)
                net.copy("l", lp.at[to_x, kk], lin.at[k, x], fs_1=to_x, fs_2=kk)
    net.wait("gram")
    gin[x] = gram[b]
    total = gin[0].astype(f32) + gin[1].astype(f32) + gin[2].astype(f32) + gin[3].astype(f32)
    quarter[...] = total.astype(bf16)
    for n, e in ((0, 1), (1, -1)):
        for kk in (k, ko):
            net.copy("col", quarter.at[n], colin.at[k, b, n], fs_0=zat(e), fs_2=kk)
    net.copy("col", quarter, colin.at[k, b], fs_2=ko)
    colin[k, b] = quarter[...]
    net.wait("l")
    pre = {}
    for m, ref in enumerate((cq_ref, cf_ref)):
        value = lin[m, 0].astype(f32)
        for n in range(1, 4):
            value = value + lin[m, n].astype(f32)
        high = value.astype(bf16)
        low = (value - high.astype(f32)).astype(bf16)
        for h in range(2):
            lanes = slice(h * 128, (h + 1) * 128)
            pre[m, h] = dot(high[:, lanes], ref[h]) + dot(low[:, lanes], ref[h])
    for c in load[9:]:
        c.wait()
    lane = lax.broadcasted_iota(jnp.int32, (16, 128), 1) // 32

    def gather_rows(group):
        net.wait(("o", group))
        for m in range(2):
            for i in (2 * group, 2 * group + 1):
                parts = []
                for n in range(4):
                    total = orv[m, n, 0, i].astype(f32)
                    for q in range(1, 4):
                        total = total + orv[m, n, q, i].astype(f32)
                    parts.append(total)
                for e in range(4):
                    block = parts[0] if e == 0 else pltpu.roll(parts[0], (128 - 32 * e) % 128, 1)
                    for n in range(1, 4):
                        turn = (32 * (n - e)) % 128
                        block = jnp.where(lane == n, pltpu.roll(parts[n], turn, 1) if turn else parts[n], block)
                    sums[m, i, e] = block

    gather_rows(0)
    gather_rows(1)
    net.wait("col")
    squares = pltpu.make_async_remote_copy(
        src_ref=sqroom,
        dst_ref=sqroom,
        send_sem=sqsem.at[0],
        recv_sem=sqsem.at[1],
        device_id=dict(fs_2=ko),
        device_id_type=MESH,
    )
    squares.wait_recv()
    squares.wait_send()
    for m in range(2):
        master_ref, copy_ref, step_ref, moment_ref, rows_ref, cols_ref = made[m::2]
        weight_old, moment_old, rows_old, cols_old = held[9 + m :: 2]
        square = sqx[m, 0]
        for n in range(1, 16):
            square = square + sqx[m, n]
        scale = jnp.sqrt(D * HW / (square + 1.0))
        twice = scale * scale
        by_row = (1.0 - stat_decay) / HW * twice
        by_col = (1.0 - stat_decay) / D * twice
        for i in range(4):
            for e in range(4):
                lanes = pl.ds(pl.multiple_of(zat(chunks[i][e]) * 128, 128), 128)
                rows_ref[:, lanes] = stat_decay * rows_old[:, lanes] + by_row * sums[m, i, e]
        for h in range(2):
            lanes = slice(h * 128, (h + 1) * 128)
            precond = scale * pre[m, h]
            moment = moment_decay * moment_old[:, lanes] + (1.0 - moment_decay) * precond
            step = moment_decay * moment + (1.0 - moment_decay) * precond
            master = weight_old[:, lanes] - learn_rate * step
            moment_ref[:, lanes] = moment
            step_ref[:, lanes] = step
            master_ref[:, lanes] = master
            copy_ref[:, lanes] = master.astype(bf16)
            for n in range(2):
                part = slice(64 * n, 64 * n + 64)
                cols_ref[h, part] = stat_decay * cols_old[h, part] + by_col * colin[m, h, n].astype(f32)
    net.drain()


def store(*refs):
    sems = refs[24]
    moves = [pltpu.make_async_copy(u, v, sems.at[n]) for n, (u, v) in enumerate(zip(refs[:12], refs[12:24]))]
    for c in moves:
        c.start()
    for c in moves:
        c.wait()


def on_device(inputs, qg, fg, fp, lb, qw, fw, qm, fm, qr, fr, qc, fc, qrr, frr, qcr, fcr):
    hbm = pl.BlockSpec(memory_space=pltpu.HBM)
    vm = pl.BlockSpec(memory_space=pltpu.VMEM)
    s = lambda shape, kind=bf16: pltpu.VMEM(shape, kind)
    given = (inputs, qg, fg, fp, lb.reshape(1, -1), qrr, frr, qcr, fcr, qw, fw, qm, fm, qr, fr, qc, fc)
    like = (qw, fw, qg, fg, qw, fw, qw, fw, qr, fr, qc, fc)
    shapes = [(v.shape if v.ndim != 2 or v.shape[1] == D else (16, 256), v.dtype) for v in like]
    made = pl.pallas_call(
        kernel,
        out_shape=tuple(pltpu.VMEM(*v) for v in shapes),
        in_specs=[hbm] * 17,
        out_specs=(vm,) * 12,
        scratch_shapes=[s(v.shape, v.dtype) for v in given]
        + [
            s((4, 128, 128)),
            s((4, 4, 128, 128)),
            s((4, 2, 128, 256)),
            s((2, 4, 4, 16, 128)),
            s((4, 2, 4, 16, 128)),
            s((4, 4, 32, 256), f32),
            s((4, 128, 256), f32),
            s((4, 128, 256), f32),
            s((4, 4, 32, 256)),
            s((7, 32, 256)),
            s((10, 32, 256)),
            s((3, 32, 256)),
            s((6, 32, 256)),
            s((4, 32, 256)),
            s((16, 32, 256)),
            s((4, 2, 4, 16, 128)),
            s((2, 4, 4, 4, 16, 128)),
            s((4, 2, 16, 256)),
            s((2, 4, 16, 256)),
            s((2, 2, 64, HEAD)),
            s((4, 2, 64, HEAD)),
            s((2, 64, HEAD)),
            s((2, 2, 2, 64, HEAD)),
            s((1, 1, 128), f32),
            s((2, 16, 1, 128), f32),
            s((31, 1, 128), f32),
            s((2, 4, 4, 16, 128), f32),
            pltpu.SemaphoreType.DMA((2,)),
            pltpu.SemaphoreType.REGULAR((2,)),
            s((TILES, 16, 128)),
            pltpu.SemaphoreType.DMA,
            pltpu.SemaphoreType.DMA((SEMS,)),
            pltpu.SemaphoreType.DMA((len(given),)),
        ],
        compiler_params=pltpu.CompilerParams(collective_id=0, has_side_effects=True),
        name="exchange",
    )(*given)
    return pl.pallas_call(
        store,
        out_shape=tuple(jax.ShapeDtypeStruct(*v) for v in shapes),
        in_specs=[vm] * 12,
        out_specs=(hbm,) * 12,
        scratch_shapes=[pltpu.SemaphoreType.DMA((12,))],
        name="store",
    )(*(pltpu.with_memory_space_constraint(v, pltpu.VMEM) for v in made))


def solution(mesh):
    split = Mesh(mesh.devices.reshape(16, 4, 2, mesh.shape["tp"]), ("fs_0", "fs_1", "fs_2", "tp"))
    both, rows, cols = P(FS, "tp"), P(FS, None), P("tp", None, None)
    return jax.shard_map(
        on_device,
        mesh=split,
        in_specs=(both,) * 4 + (P("tp"),) + (both,) * 4 + (rows,) * 2 + (cols,) * 2 + (rows,) * 2 + (cols,) * 2,
        out_specs=(both,) * 8 + (rows,) * 2 + (cols,) * 2,
        check_vma=False,
    )
```

```python
import jax
import jax.numpy as jnp
from jax import lax
from jax.experimental import pallas as pl
from jax.experimental.pallas import tpu as pltpu
from jax.sharding import Mesh
from jax.sharding import PartitionSpec as P

D = 2048
HW = 1024
HEAD = 128
FS = ("fs_0", "fs_1", "fs_2")
MESH = pl.DeviceIdType.MESH
SEMS = 27
TILES = 698

stat_decay = 0.9
moment_decay = 0.9
learn_rate = 0.02
highest = lax.Precision.HIGHEST
f32 = jnp.float32
bf16 = jnp.bfloat16


class Net:
    def __init__(self, send, recv, room, other):
        self.send, self.recv, self.room, self.other = send, recv, room, other
        self.names, self.sent, self.waited = {}, {}, {}

    def sem(self, name):
        return self.recv.at[self.names.setdefault(name, len(self.names))]

    def copy(self, name, src, dst, count=True, **where):
        pltpu.make_async_remote_copy(
            src_ref=src,
            dst_ref=dst,
            send_sem=self.send,
            recv_sem=self.sem(name),
            device_id=where,
            device_id_type=MESH,
        ).start()
        size = src.dtype.itemsize
        for n in src.shape:
            size *= n
        assert size % 4096 == 0
        if count:
            self.sent[name] = self.sent.get(name, 0) + size // 4096

    def tiles(self, sem, tiles):
        room = self.room.at[pl.ds(0, tiles)]
        return pltpu.make_async_remote_copy(
            src_ref=room,
            dst_ref=room,
            send_sem=self.send,
            recv_sem=sem,
            device_id=self.other,
            device_id_type=MESH,
        )

    def wait(self, name):
        assert name not in self.waited
        self.waited[name] = self.sent[name]
        self.tiles(self.sem(name), self.sent[name]).wait_recv()

    def drain(self):
        assert self.waited == self.sent
        total = sum(self.sent.values())
        assert (len(self.names), total) == (SEMS, TILES), (len(self.names), total)
        self.tiles(self.recv.at[0], total).wait_send()


def dot(a, b):
    return jnp.dot(a, b, preferred_element_type=f32)


def kernel(
    *refs,
):
    given, refs = refs[:17], refs[17:]
    made, refs = refs[:12], refs[12:]
    held, refs = refs[:17], refs[17:]
    x_ref, qg_ref, fg_ref, fp_ref, lb_ref, rq_ref, rf_ref, cq_ref, cf_ref = held[:9]
    (
    xt, xx, gx, rpack, rin, pmine, pout, pin, gp, rd, ru, sb, rf, gz, gc, o, orv, lp, lin, gram, gin, quarter, colin, sq, sqx, sqroom, sums, sqsem, tokens,
    room, send, recv, loads,
    ) = refs
    z, x, k, y = (lax.axis_index(n) for n in ("fs_0", "fs_1", "fs_2", "tp"))
    ko, b = 1 - k, lax.rem(z, 2)
    at = lambda v, n, m: lax.rem(v + n + m, m)
    ym, yp, y2 = at(y, -1, 4), at(y, 1, 4), at(y, 2, 4)
    zat = lambda n: at(z, n, 16)
    net = Net(send, recv, room, dict(fs_2=ko))
    steps = (2, 1, 3)
    plane = [
        (dx, dy, kk)
        for dx, dy in ((2, 2), (1, 2), (3, 2), (2, 1), (2, 3), (1, 1), (3, 3), (1, 3), (3, 1), (2, 0), (0, 2), (1, 0), (0, 1), (3, 0), (0, 3), (0, 0))
        for kk in (k, ko)
        if (dx, dy) != (0, 0) or kk is ko
    ]

    load = [pltpu.make_async_copy(u, v, loads.at[n]) for n, (u, v) in enumerate(zip(given, held))]
    load[0].start()
    barrier = pltpu.get_barrier_semaphore()
    partners = [dict(fs_1=at(x, d, 4)) for d in steps]
    partners += [dict(tp=at(y, d, 4)) for d in steps]
    partners += [dict(fs_0=zat(n)) for n in (1, -1)] + [dict(fs_2=ko)]
    for who in partners:
        pl.semaphore_signal(barrier, inc=1, device_id=who, device_id_type=MESH)

    for c in load[1:9]:
        c.start()
    load[0].wait()
    for n in range(4):
        turned = x_ref[:, n * 128 : (n + 1) * 128].T
        for q in range(4):
            xt[q, n * 32 : (n + 1) * 32] = turned[q * 32 : (q + 1) * 32]
    xx[y, x] = xt[x]
    for c in load[1:5]:
        c.wait()
    gx[x, 0] = qg_ref[...]
    gate = jax.nn.sigmoid(fp_ref[...].astype(f32))
    gx[x, 1] = (fg_ref[...].astype(f32) * (1.0 - lb_ref[...]) * gate * (1.0 - gate)).astype(bf16)
    pl.semaphore_wait(barrier, len(partners))

    for d in steps:
        net.copy(("x", d), xt.at[at(x, d, 4)], xx.at[y, x], fs_1=at(x, d, 4))

    def ysend(n):
        for d in steps:
            net.copy(("y", d), xx.at[y, n], xx.at[y, n], tp=at(y, d, 4))

    ysend(x)

    def token(n):
        for e in (1, -1):
            pl.semaphore_signal(tokens.at[n], inc=1, device_id=dict(fs_0=zat(e)), device_id_type=MESH)

    token(0)
    for c in load[9:]:
        c.start()
    halves = (pl.ds(0, 64), pl.ds(64, 64))

    def gcopy(name, n, m, h, d):
        net.copy(name, gx.at[n, m, h], gx.at[n, m, h], fs_1=at(x, d, 4))

    for i, h in enumerate(halves):
        gcopy(("gq", i), x, 0, h, 1)
        gcopy(("gf", i), x, 1, h, -1)
    for h in halves:
        gcopy("g", x, 1, h, 1)
        gcopy("g", x, 0, h, -1)
    for c in load[5:9]:
        c.wait()
    for m, ref in enumerate((rq_ref, rf_ref)):
        for n in range(4):
            wide = ref[:, n * 512 : (n + 1) * 512].astype(f32)
            for q in range(4):
                strips = [wide[:, w * 128 + q * 32 : w * 128 + (q + 1) * 32] for w in range(4)]
                rpack[m, q, n] = jnp.concatenate(strips, axis=1).astype(bf16)
    rin[x, k] = rpack[k, x]
    net.copy("r", rpack.at[ko, x], rin.at[x, k], fs_2=ko)
    for d in (1, 3, 2):
        net.wait(("x", d))
        ysend(at(x, -d, 4))

    def product(j, a):
        lhs = jnp.concatenate([xx[a, n] for n in range(4)], axis=1)
        pout[a] = dot(lhs, gx[:, ko].reshape(512, 256))
        pmine[a] = dot(lhs, gx[:, k].reshape(512, 256)).reshape(4, 32, 256)
        net.copy(("p", j), pout.at[a], pin.at[a], fs_2=ko)

    def scatter(j, a):
        net.wait(("p", j))
        total = pmine[a] + pin[a].reshape(4, 32, 256)
        pmine[a] = total
        gp[a] = total.astype(bf16)
        for q in range(4):
            t = 4 * a + q
            d = at(t, -z, 16)
            up = (d == 4) | (d == 5) | (d == 7) | (d == 8)
            down = (d == 9) | (d == 11) | (d == 12)
            direct = (d == 1) | (d == 2) | (d == 3) | (d == 13) | (d == 14) | (d == 15)

            @pl.when(up | down)
            def _():
                slot = d - jnp.where(up, 4, 3)
                relay = lax.rem(t + jnp.where(up, 10, 6), 16)
                net.copy("u", gp.at[a, q], ru.at[slot], count=False, fs_0=relay)

            @pl.when(direct)
            def _():
                net.copy("s", gp.at[a, q], rd.at[lax.rem(d + 3, 16)], count=False, fs_0=t)

    for i, h in enumerate(halves):
        net.wait(("gq", i))
        gcopy("g", at(x, -1, 4), 0, h, 1)
        net.wait(("gf", i))
        gcopy("g", at(x, 1, 4), 1, h, -1)
    net.wait("g")
    pl.semaphore_wait(tokens.at[0], 2)
    token(1)
    product(0, y)
    net.wait(("y", 1))
    product(1, ym)
    net.wait(("y", 3))
    product(2, yp)
    net.wait(("y", 2))
    product(3, y2)
    pl.semaphore_wait(tokens.at[1], 2)
    scatter(0, y)
    scatter(1, ym)
    scatter(2, yp)
    scatter(3, y2)
    for dx in steps:
        for m, kk in ((k, k), (ko, ko)):
            net.copy("r", rpack.at[m, at(x, dx, 4)], rin.at[x, k], fs_1=at(x, dx, 4), fs_2=kk)
    net.sent["s"], net.sent["u"] = 6 * 4, 7 * 4
    net.wait("u")
    part = lambda t: pmine[t // 4, lax.rem(t, 4)]
    net.wait("s")
    for n, e, slots in ((0, 6, (0, 1, 3, 4)), (1, -6, (6, 8, 9))):
        total = part(zat(e))
        for i in slots:
            total = total + ru[i].astype(f32)
        sb[n] = total.astype(bf16)
        net.copy("f", sb.at[n], rf.at[2 + 2 * n], fs_0=zat(e))
        net.copy("f", sb.at[n], rf.at[3 + 2 * n], fs_0=zat(2 * e))
    total = part(z)
    for i in (0, 1, 2, 4, 5, 6):
        total = total + rd[i].astype(f32)
    sb[2] = total.astype(bf16)
    net.copy("f", sb.at[2], rf.at[0], fs_0=zat(6))
    net.copy("f", sb.at[2], rf.at[1], fs_0=zat(-6))
    net.wait("f")

    def joined(mid, above, below):
        return (mid.astype(f32) + above.astype(f32) + below.astype(f32)).astype(bf16)

    mine = joined(sb[2], rf[4], rf[2])
    gc[z] = mine
    gz[x] = mine
    gc[zat(6)] = joined(rf[1], rf[5], sb[0])
    gc[zat(-6)] = joined(rf[0], sb[1], rf[3])

    chunks = ((0, 6, -6, 1), (7, -5, -1, 5), (-7, 2, -8, -4), (-2, 4, 3, -3))
    for d in steps:
        net.copy("gz", gz.at[x], gz.at[x], fs_1=at(x, d, 4))
    for name, n, held_here in (
        ("first", 1, (0, 6, -6)), ("first", -1, (0, 6, -6)), ("last", 3, (0,)), ("last", -3, (0,)),
        ("last", 2, (0, 6, -6)), ("last", -2, (0, -6)),
    ):
        for e in held_here:
            net.copy(("z", name), gc.at[zat(e)], gc.at[zat(e)], fs_0=zat(n))
    net.wait("r")
    net.wait(("z", "first"))
    net.wait("gz")
    rows = gz[...].reshape(128, 256)

    def outer(i):
        cols = jnp.concatenate([gc[zat(e)] for e in chunks[i]], axis=0)
        block = lax.dot_general(rows, cols, (((1,), (1,)), ((), ())), preferred_element_type=f32).astype(bf16)
        for q in range(8):
            o[q // 2, q % 2, i] = block[q * 16 : (q + 1) * 16]

    def osend(group, h):
        orv[k, x, y, h] = o[x, k, h]
        for dx, dy, kk in plane:
            to_x, to_y = at(x, dx, 4), at(y, dy, 4)
            net.copy(("o", group), o.at[to_x, kk, h], orv.at[k, x, y, h], fs_1=to_x, tp=to_y, fs_2=kk)

    outer(0)
    outer(1)
    osend(0, pl.ds(0, 2))
    net.wait(("z", "last"))
    whole = gc[...].reshape(512, 256)
    for h in range(2):
        lanes = slice(h * 128, (h + 1) * 128)
        turned = whole[:, lanes]
        both = lax.dot_general(turned, turned, (((0,), (0,)), ((), ())), preferred_element_type=f32).astype(bf16)
        gram[h, 0] = both[:64]
        gram[h, 1] = both[64:]
    for d in steps:
        net.copy("gram", gram.at[b], gin.at[x], fs_1=at(x, d, 4))
    wide = whole.astype(f32)
    square = jnp.sum((wide * wide).reshape(64, 8, 256), axis=0)
    square = jnp.sum(square, axis=(0, 1), keepdims=True)
    sq[0] = jnp.broadcast_to(square, (1, 128))
    outer(2)
    outer(3)
    sqx[k, 4 * x + y] = sq[0]
    for dx, dy, kk in plane:
        pltpu.make_async_remote_copy(
            src_ref=sq.at[0],
            dst_ref=sqx.at[k, 4 * x + y],
            send_sem=sqsem.at[0],
            recv_sem=sqsem.at[1],
            device_id=dict(fs_1=at(x, dx, 4), tp=at(y, dy, 4), fs_2=kk),
            device_id_type=MESH,
        ).start()
    osend(1, pl.ds(2, 2))
    roots = rin[...].reshape(8, 4, 16, 128)
    roots = jnp.concatenate(
        [jnp.concatenate([roots[q, n] for n in range(4)], axis=1) for q in range(8)], axis=0
    )
    left = dot(roots, whole)
    lp[...] = left.reshape(4, 2, 16, 256).astype(bf16)
    lin[k, x] = lp[x, k]
    for dx in (2, 1, 3, 0):
        for kk in (k, ko):
            if dx or kk is ko:
                to_x = at(x, dx, 4)
                net.copy("l", lp.at[to_x, kk], lin.at[k, x], fs_1=to_x, fs_2=kk)
    net.wait("gram")
    gin[x] = gram[b]
    total = gin[0].astype(f32) + gin[1].astype(f32) + gin[2].astype(f32) + gin[3].astype(f32)
    quarter[...] = total.astype(bf16)
    for n, e in ((0, 1), (1, -1)):
        for kk in (k, ko):
            net.copy("col", quarter.at[n], colin.at[k, b, n], fs_0=zat(e), fs_2=kk)
    net.copy("col", quarter, colin.at[k, b], fs_2=ko)
    colin[k, b] = quarter[...]
    net.wait("l")
    pre = {}
    for m, ref in enumerate((cq_ref, cf_ref)):
        value = lin[m, 0].astype(f32)
        for n in range(1, 4):
            value = value + lin[m, n].astype(f32)
        high = value.astype(bf16)
        low = (value - high.astype(f32)).astype(bf16)
        for h in range(2):
            lanes = slice(h * 128, (h + 1) * 128)
            pre[m, h] = dot(high[:, lanes], ref[h]) + dot(low[:, lanes], ref[h])
    for c in load[9:]:
        c.wait()
    lane = lax.broadcasted_iota(jnp.int32, (16, 128), 1) // 32

    def gather_rows(group):
        net.wait(("o", group))
        for m in range(2):
            for i in (2 * group, 2 * group + 1):
                parts = []
                for n in range(4):
                    total = orv[m, n, 0, i].astype(f32)
                    for q in range(1, 4):
                        total = total + orv[m, n, q, i].astype(f32)
                    parts.append(total)
                for e in range(4):
                    block = parts[0] if e == 0 else pltpu.roll(parts[0], (128 - 32 * e) % 128, 1)
                    for n in range(1, 4):
                        turn = (32 * (n - e)) % 128
                        block = jnp.where(lane == n, pltpu.roll(parts[n], turn, 1) if turn else parts[n], block)
                    sums[m, i, e] = block

    gather_rows(0)
    gather_rows(1)
    net.wait("col")
    squares = pltpu.make_async_remote_copy(
        src_ref=sqroom,
        dst_ref=sqroom,
        send_sem=sqsem.at[0],
        recv_sem=sqsem.at[1],
        device_id=dict(fs_2=ko),
        device_id_type=MESH,
    )
    squares.wait_recv()
    squares.wait_send()
    for m in range(2):
        master_ref, copy_ref, step_ref, moment_ref, rows_ref, cols_ref = made[m::2]
        weight_old, moment_old, rows_old, cols_old = held[9 + m :: 2]
        square = sqx[m, 0]
        for n in range(1, 16):
            square = square + sqx[m, n]
        scale = jnp.sqrt(D * HW / (square + 1.0))
        twice = scale * scale
        by_row = (1.0 - stat_decay) / HW * twice
        by_col = (1.0 - stat_decay) / D * twice
        for i in range(4):
            for e in range(4):
                lanes = pl.ds(pl.multiple_of(zat(chunks[i][e]) * 128, 128), 128)
                rows_ref[:, lanes] = stat_decay * rows_old[:, lanes] + by_row * sums[m, i, e]
        for h in range(2):
            lanes = slice(h * 128, (h + 1) * 128)
            precond = scale * pre[m, h]
            moment = moment_decay * moment_old[:, lanes] + (1.0 - moment_decay) * precond
            step = moment_decay * moment + (1.0 - moment_decay) * precond
            master = weight_old[:, lanes] - learn_rate * step
            moment_ref[:, lanes] = moment
            step_ref[:, lanes] = step
            master_ref[:, lanes] = master
            copy_ref[:, lanes] = master.astype(bf16)
            for n in range(2):
                part = slice(64 * n, 64 * n + 64)
                cols_ref[h, part] = stat_decay * cols_old[h, part] + by_col * colin[m, h, n].astype(f32)
    net.drain()


def store(*refs):
    sems = refs[24]
    moves = [pltpu.make_async_copy(u, v, sems.at[n]) for n, (u, v) in enumerate(zip(refs[:12], refs[12:24]))]
    for c in moves:
        c.start()
    for c in moves:
        c.wait()


def on_device(inputs, qg, fg, fp, lb, qw, fw, qm, fm, qr, fr, qc, fc, qrr, frr, qcr, fcr):
    hbm = pl.BlockSpec(memory_space=pltpu.HBM)
    vm = pl.BlockSpec(memory_space=pltpu.VMEM)
    s = lambda shape, kind=bf16: pltpu.VMEM(shape, kind)
    given = (inputs, qg, fg, fp, lb.reshape(1, -1), qrr, frr, qcr, fcr, qw, fw, qm, fm, qr, fr, qc, fc)
    like = (qw, fw, qg, fg, qw, fw, qw, fw, qr, fr, qc, fc)
    shapes = [(v.shape if v.ndim != 2 or v.shape[1] == D else (16, 256), v.dtype) for v in like]
    made = pl.pallas_call(
        kernel,
        out_shape=tuple(pltpu.VMEM(*v) for v in shapes),
        in_specs=[hbm] * 17,
        out_specs=(vm,) * 12,
        scratch_shapes=[s(v.shape, v.dtype) for v in given]
        + [
            s((4, 128, 128)),
            s((4, 4, 128, 128)),
            s((4, 2, 128, 256)),
            s((2, 4, 4, 16, 128)),
            s((4, 2, 4, 16, 128)),
            s((4, 4, 32, 256), f32),
            s((4, 128, 256), f32),
            s((4, 128, 256), f32),
            s((4, 4, 32, 256)),
            s((7, 32, 256)),
            s((10, 32, 256)),
            s((3, 32, 256)),
            s((6, 32, 256)),
            s((4, 32, 256)),
            s((16, 32, 256)),
            s((4, 2, 4, 16, 128)),
            s((2, 4, 4, 4, 16, 128)),
            s((4, 2, 16, 256)),
            s((2, 4, 16, 256)),
            s((2, 2, 64, HEAD)),
            s((4, 2, 64, HEAD)),
            s((2, 64, HEAD)),
            s((2, 2, 2, 64, HEAD)),
            s((1, 1, 128), f32),
            s((2, 16, 1, 128), f32),
            s((31, 1, 128), f32),
            s((2, 4, 4, 16, 128), f32),
            pltpu.SemaphoreType.DMA((2,)),
            pltpu.SemaphoreType.REGULAR((2,)),
            s((TILES, 16, 128)),
            pltpu.SemaphoreType.DMA,
            pltpu.SemaphoreType.DMA((SEMS,)),
            pltpu.SemaphoreType.DMA((len(given),)),
        ],
        compiler_params=pltpu.CompilerParams(collective_id=0, has_side_effects=True),
        name="exchange",
    )(*given)
    return pl.pallas_call(
        store,
        out_shape=tuple(jax.ShapeDtypeStruct(*v) for v in shapes),
        in_specs=[vm] * 12,
        out_specs=(hbm,) * 12,
        scratch_shapes=[pltpu.SemaphoreType.DMA((12,))],
        name="store",
    )(*(pltpu.with_memory_space_constraint(v, pltpu.VMEM) for v in made))


def solution(mesh):
    split = Mesh(mesh.devices.reshape(16, 4, 2, mesh.shape["tp"]), ("fs_0", "fs_1", "fs_2", "tp"))
    both, rows, cols = P(FS, "tp"), P(FS, None), P("tp", None, None)
    return jax.shard_map(
        on_device,
        mesh=split,
        in_specs=(both,) * 4 + (P("tp"),) + (both,) * 4 + (rows,) * 2 + (cols,) * 2 + (rows,) * 2 + (cols,) * 2,
        out_specs=(both,) * 8 + (rows,) * 2 + (cols,) * 2,
        check_vma=False,
    )
```
